32 devices in a mesh: fs: 8 (over z, core), tp: 4 (over y, x).
Axes of the slice: x: 2, y: 2, z: 4, core: 2. Of those that a mesh axis runs over, the one named last changes fastest.
Arguments:
- late_input: bfloat16 [1024, 2048], P('fs'), may hold values from -6 to 6
- early_input: bfloat16 [1024, 2048], P('fs'), may hold values from -6 to 6
- early_mid: bfloat16 [1024, 2048], P('fs'), may hold values from -6 to 6
- cotangent: bfloat16 [1024, 2048], P('fs'), may hold values from -6 to 6
- gain_first: float32 [2048], replicated, may hold values from 0.1 to 1.9
- gain_second: float32 [2048], replicated, may hold values from 0.1 to 1.9
- gate_first: bfloat16 [2048, 2816], P('fs', 'tp'), may hold values from -0.125 to 0.125
- up_first: bfloat16 [2048, 2816], P('fs', 'tp'), may hold values from -0.125 to 0.125
- down_first: bfloat16 [2816, 2048], P('tp', 'fs'), may hold values from -0.109375 to 0.109375
- gate_second: bfloat16 [2048, 2816], P('fs', 'tp'), may hold values from -0.125 to 0.125
- up_second: bfloat16 [2048, 2816], P('fs', 'tp'), may hold values from -0.125 to 0.125
- down_second: bfloat16 [2816, 2048], P('tp', 'fs'), may hold values from -0.109375 to 0.109375
- sum_gate_first: float32 [2048, 2816], P('fs', 'tp'), may hold values from -128 to 128
- sum_up_first: float32 [2048, 2816], P('fs', 'tp'), may hold values from -128 to 128
- sum_down_first: float32 [2816, 2048], P('tp', 'fs'), may hold values from -128 to 128
- sum_gate_second: float32 [2048, 2816], P('fs', 'tp'), may hold values from -128 to 128
- sum_up_second: float32 [2048, 2816], P('fs', 'tp'), may hold values from -128 to 128
- sum_down_second: float32 [2816, 2048], P('tp', 'fs'), may hold values from -128 to 128
Outputs:
- late_mid: bfloat16 [1024, 2048], P('fs')
- late_out: bfloat16 [1024, 2048], P('fs')
- input_grad: bfloat16 [1024, 2048], P('fs')
- new_gate_first: float32 [2048, 2816], P('fs', 'tp')
- new_up_first: float32 [2048, 2816], P('fs', 'tp')
- new_down_first: float32 [2816, 2048], P('tp', 'fs')
- new_gate_second: float32 [2048, 2816], P('fs', 'tp')
- new_up_second: float32 [2048, 2816], P('fs', 'tp')
- new_down_second: float32 [2816, 2048], P('tp', 'fs')
The draws below stay inside these ranges and needn't reach their ends.
All inputs are finite; a program needn't handle non-finite values.
Results may differ from the reference program's by a relative error of at most 0.015.
Values may be sent and summed in bfloat16 or wider, within the bound.
A program may use at most 128 MiB of HBM per device.

```python
import jax
import jax.numpy as jnp
from jax import lax

D = 2048
FF = 2816
TOKENS = 1024
N_TP = 4


def with_spikes(result, own_key, source, target, parts, factor):
    def block_of(dim):
        return (jnp.arange(result.shape[dim]) // (result.shape[dim] // parts)).reshape((-1,) + (1,) * (result.ndim - 1 - dim))

    near = jax.random.permutation(own_key, parts)[block_of(target)]
    other_side = (block_of(target) + parts // 2) % parts
    return jnp.where((block_of(source) == near) | (block_of(source) == other_side), factor * result, result)


def level_of(key, shape, shards, smallest, top_value):
    factor_of, own = 1.0, jax.random.fold_in(key, 6)
    for dim, shards_of in shards:
        steps = jnp.exp(jax.random.uniform(jax.random.fold_in(own, dim), (shards_of,), jnp.float32, smallest / len(shards), top_value / len(shards)))
        factor_of = factor_of * jnp.repeat(steps, shape[dim] // shards_of).reshape([-1 if axis == dim else 1 for axis in range(len(shape))])
    return factor_of


def bell_draw(own_key, dims, width, most, split=(), held_as=jnp.bfloat16):
    array = jax.random.normal(own_key, dims, jnp.float32) * width
    if len(split) > 0:
        array = level_of(own_key, dims, split, -0.22, 0.18) * array
    return jnp.clip(array, min=-most, max=most).astype(held_as)


def bell_draw_with(rng, dims, width, most, pieces, heavy, dtype=jnp.bfloat16):
    values = width * jax.random.normal(rng, dims, jnp.float32)
    if pieces:
        values = values * level_of(rng, dims, pieces, -0.22, 0.18)
    return jnp.clip(with_spikes(values, jax.random.fold_in(rng, 3), *heavy), -most, most).astype(dtype)


def setup_inputs(seed: int = 0) -> dict:
    streams_of = jax.random.split(jax.random.key(seed), 19)
    late_input = bell_draw(streams_of[0], (TOKENS, D), 1.0, 6.0, ((0, 8),))
    early_input = bell_draw(streams_of[1], (TOKENS, D), 1.0, 6.0, ((0, 8),))
    early_mid = bell_draw(streams_of[2], (TOKENS, D), 1.0, 6.0, ((0, 8),))
    cotangent = bell_draw_with(streams_of[3], (TOKENS, D), 1.0, 6.0, ((0, 8),), (0, 1, 8, 2.0))
    gain_first = jnp.clip(1.0 + 0.18 * jax.random.normal(streams_of[4], (D,), jnp.float32), 0.1, 1.9)
    gain_second = jnp.clip(1.0 + 0.18 * jax.random.normal(streams_of[5], (D,), jnp.float32), 0.1, 1.9)
    gate_first = bell_draw(streams_of[6], (D, FF), D ** -0.5, 0.125, ((0, 8), (1, 4)))
    up_first = bell_draw(streams_of[7], (D, FF), D ** -0.5, 0.125, ((0, 8), (1, 4)))
    down_first = bell_draw(streams_of[8], (FF, D), FF ** -0.5, 0.109375, ((0, 4), (1, 8)))
    gate_second = bell_draw(streams_of[9], (D, FF), D ** -0.5, 0.125, ((0, 8), (1, 4)))
    up_second = bell_draw(streams_of[10], (D, FF), D ** -0.5, 0.125, ((0, 8), (1, 4)))
    down_second = bell_draw(streams_of[11], (FF, D), FF ** -0.5, 0.109375, ((0, 4), (1, 8)))
    sum_gate_first = bell_draw(streams_of[12], (D, FF), (0.25 * TOKENS ** 0.5), 128.0, ((0, 8), (1, 4)), jnp.float32)
    sum_up_first = bell_draw(streams_of[13], (D, FF), (0.25 * TOKENS ** 0.5), 128.0, ((0, 8), (1, 4)), jnp.float32)
    sum_down_first = bell_draw(streams_of[14], (FF, D), (0.25 * TOKENS ** 0.5), 128.0, ((0, 4), (1, 8)), jnp.float32)
    sum_gate_second = bell_draw(streams_of[15], (D, FF), (0.25 * TOKENS ** 0.5), 128.0, ((0, 8), (1, 4)), jnp.float32)
    sum_up_second = bell_draw(streams_of[16], (D, FF), (0.25 * TOKENS ** 0.5), 128.0, ((0, 8), (1, 4)), jnp.float32)
    sum_down_second = bell_draw(streams_of[17], (FF, D), (0.25 * TOKENS ** 0.5), 128.0, ((0, 4), (1, 8)), jnp.float32)
    return {"late_input": late_input, "early_input": early_input, "early_mid": early_mid, "cotangent": cotangent, "gain_first": gain_first, "gain_second": gain_second, "gate_first": gate_first, "up_first": up_first, "down_first": down_first, "gate_second": gate_second, "up_second": up_second, "down_second": down_second, "sum_gate_first": sum_gate_first, "sum_up_first": sum_up_first, "sum_down_first": sum_down_first, "sum_gate_second": sum_gate_second, "sum_up_second": sum_up_second, "sum_down_second": sum_down_second}


norm_eps = 1e-06

def normalize(values, gain_vector):
    widened = values.astype(jnp.float32)
    factor = lax.rsqrt(lax.optimization_barrier(jnp.mean(widened * widened, axis=-1, keepdims=True)) + norm_eps)
    normed = (widened * factor * gain_vector.astype(jnp.float32)).astype(jnp.bfloat16)
    return (widened, factor, normed)

def groupwise(operands, part_count):
    part_width = operands[0][0].shape[1] // part_count
    running = jnp.zeros((operands[0][0].shape[0], operands[0][1].shape[1]), jnp.float32)
    for part_index in range(part_count):
        lower = part_index * part_width
        product = jnp.zeros_like(running)
        for left_rows, right_cols in operands:
            product = product + jnp.dot(left_rows[:, lower:lower + part_width], right_cols[lower:lower + part_width], preferred_element_type=jnp.float32)
        rounded = lax.optimization_barrier(product.astype(jnp.bfloat16))
        running = running + rounded.astype(jnp.float32)
    return running

def block_forward(values, gain_vector, w_gate, w_up, w_down):
    widened, factor, normed = normalize(values, gain_vector)
    gate_pre = jnp.dot(normed, w_gate, preferred_element_type=jnp.float32)
    up_pre = jnp.dot(normed, w_up, preferred_element_type=jnp.float32)
    hidden = (jax.nn.silu(gate_pre) * up_pre).astype(jnp.bfloat16)
    branch = groupwise(((hidden, w_down),), N_TP)
    return (widened + 0.5 * branch).astype(jnp.bfloat16)

def block_backward(values, cotangent, gain_vector, w_gate, w_up, w_down):
    widened, factor, normed = normalize(values, gain_vector)
    gate_pre = jnp.dot(normed, w_gate, preferred_element_type=jnp.float32)
    up_pre = jnp.dot(normed, w_up, preferred_element_type=jnp.float32)
    sigmoid_gate = jax.nn.sigmoid(gate_pre)
    activated = gate_pre * sigmoid_gate
    hidden = (activated * up_pre).astype(jnp.bfloat16)
    hidden_grad = 0.5 * jnp.dot(cotangent, w_down.T, preferred_element_type=jnp.float32)
    gate_grad = (hidden_grad * up_pre * sigmoid_gate * (1.0 + gate_pre * (1.0 - sigmoid_gate))).astype(jnp.bfloat16)
    up_grad = (hidden_grad * activated).astype(jnp.bfloat16)
    normed_grad = groupwise(((gate_grad, w_gate.T), (up_grad, w_up.T)), N_TP)
    scaled = normed_grad * gain_vector.astype(jnp.float32)
    unit_rows = widened * factor
    rows_grad = cotangent.astype(jnp.float32) + factor * (scaled - unit_rows * lax.optimization_barrier(jnp.mean(scaled * unit_rows, axis=-1, keepdims=True)))
    grad_gate = jnp.dot(normed.T, gate_grad, preferred_element_type=jnp.float32)
    grad_up = jnp.dot(normed.T, up_grad, preferred_element_type=jnp.float32)
    grad_down = 0.5 * jnp.dot(hidden.T, cotangent, preferred_element_type=jnp.float32)
    return (rows_grad, (grad_gate, grad_up, grad_down))

def reference(late_input, early_input, early_mid, cotangent, gain_first, gain_second, gate_first, up_first, down_first, gate_second, up_second, down_second, sum_gate_first, sum_up_first, sum_down_first, sum_gate_second, sum_up_second, sum_down_second):
    late_mid = block_forward(late_input, gain_first, gate_first, up_first, down_first)
    late_out = block_forward(late_mid, gain_second, gate_second, up_second, down_second)
    mid_grad, grads_second = block_backward(early_mid, cotangent, gain_second, gate_second, up_second, down_second)
    mid_grad = mid_grad.astype(jnp.bfloat16)
    rows_grad, grads_first = block_backward(early_input, mid_grad, gain_first, gate_first, up_first, down_first)
    return (late_mid, late_out, rows_grad.astype(jnp.bfloat16), sum_gate_first + grads_first[0], sum_up_first + grads_first[1], sum_down_first + grads_first[2], sum_gate_second + grads_second[0], sum_up_second + grads_second[1], sum_down_second + grads_second[2])
```

```python
import functools

import jax
import jax.numpy as jnp
from jax import lax
from jax.experimental import pallas as pl
from jax.experimental.pallas import tpu as pltpu
from jax.sharding import PartitionSpec as P

norm_eps = 1e-06
CORES = 2
TP = 4
PLANES = 4

NT = (((1,), (1,)), ((), ()))
NN = (((1,), (0,)), ((), ()))
TN = (((0,), (0,)), ((), ()))


def mm(left, right, dims):
    return lax.dot_general(left, right, dims, preferred_element_type=jnp.float32)


def norm_parts(rows):
    wide = rows.astype(jnp.float32)
    factor = lax.rsqrt(jnp.mean(wide * wide, axis=-1, keepdims=True) + norm_eps)
    return wide, factor


def step_kernel(
    late_in, mid_in, cot_in, early_in, gain2, gain1, w2, w1,
    out_rows, g20, g21, g22, g10, g11, g12,
    weights, acts, late, normed, late_normed, pieces, pieces_in, cols_in,
    part, part_in2, part_in1, late_part, late_part_in, sent, back_rows, done_rows,
    acc, late_acc, late_hid, send_sems, recv_sems, local_sems, ack,
):
    f, t = lax.axis_index("fs"), lax.axis_index("tp")
    z, core = f // CORES, f % CORES
    peer = 1 - core
    inner = (z == 1) | (z == 2)
    outer = (z == 0) | (z == 3)
    near, upper = (z // 2) * 3, z // 2
    q = late_in.shape[0] // TP
    rows = PLANES * q
    half = 2 * q
    width = w2.shape[1]
    hidden = w2.shape[0] // 3
    tile = TP * half
    grads = ((g20, g21, g22), (g10, g11, g12))
    shards = (w2, w1)
    gains = (gain2, gain1)
    ids = {}

    def sem(name):
        return ids.setdefault(name, len(ids))

    def column(mask):
        x, y = t % 2, t // 2
        gx, gy = mask % 2, mask // 2
        x = x + gx - 2 * x * gx
        y = y + gy - 2 * y * gy
        return y * 2 + x

    def device(zz, cc, tt):
        return (zz * CORES + cc, tt)

    def remote(src, dst, index, where):
        return pltpu.make_async_remote_copy(
            src_ref=src, dst_ref=dst, send_sem=send_sems.at[index],
            recv_sem=recv_sems.at[index], device_id=where,
            device_id_type=pl.DeviceIdType.MESH,
        )

    def local(src, dst, index):
        return pltpu.make_async_copy(src, dst, local_sems.at[index])

    def own_quarter(tt):
        return pl.ds(pl.multiple_of(tt * q, q), q)

    def feature(slot, other):
        v = slot + (1 - slot // 2) * (1 - 2 * slot)
        zs = v + upper * (3 - 2 * v)
        cc = core + other - 2 * core * other
        return pl.ds(pl.multiple_of((zs * CORES + cc) * width, width), width)

    barrier = pltpu.get_barrier_semaphore()
    friends = [device((z + k) % PLANES, core, t) for k in range(1, PLANES)]
    friends += [device(z, peer, t)] + [device(z, core, column(m)) for m in range(1, TP)]
    for friend in friends:
        pl.semaphore_signal(barrier, inc=1, device_id=friend, device_id_type=pl.DeviceIdType.MESH)
    pl.semaphore_wait(barrier, len(friends))

    mine = own_quarter(t)
    z_items = []
    for name, src, to in (
        ("m", mid_in, lambda s: acts.at[0, 0, pl.ds(s * q, q)]),
        ("c", cot_in, lambda s: acts.at[1, 0, pl.ds(s * q, q)]),
    ):
        z_items.append((name, src.at[mine], to))
    z_items.append(("w0", w2, lambda s: weights.at[0, s]))
    z_items.append(("e", early_in.at[mine], lambda s: acts.at[2, 0, pl.ds(s * q, q)]))
    z_items.append(("l", late_in.at[mine], lambda s: late.at[0, 0, pl.ds(s * q, q)]))
    z_items.append(("w1", w1, lambda s: weights.at[1, s]))
    z_base = {}
    for name, _, _ in z_items:
        z_base[name] = sem((name, 0))
        for s in range(1, 4):
            sem((name, s))

    def z_copy(item, s, where):
        name, src, to = item
        return remote(src, to(s), z_base[name] + s, where)

    first_target = device(1 + upper, core, t)
    second_target = device(2 - upper, core, t)
    mid_target = device(3 - z, core, t)

    def outer_sends():
        out = []
        for item in z_items:
            out.append(z_copy(item, 1, first_target))
            if item[0] != "l":
                out.append(z_copy(item, 3, second_target))
        return out

    def inner_sends():
        return [z_copy(item, 2, mid_target) for item in z_items if item[0] != "l"]

    out_dev = device(near, core, t)

    def grad_back(b, j):
        return remote(sent[3 * b + j], grads[b][j], sem(("g", b, j)), out_dev)

    def row_source(k):
        return (late.at[1, 0], done_rows.at[0], done_rows.at[1])[k]

    def rows_back(k):
        return remote(row_source(k).at[pl.ds(q, q)], back_rows.at[k], sem(("r", k)), out_dev)

    def deliver(k, m, src):
        return remote(src, out_rows.at[k, mine], sem(("d", k, m)), device(z, core, column(m)))

    def deliver_wait(k, m):
        other = column(m)
        dst = out_rows.at[k, own_quarter(other)]
        remote(dst, dst, sem(("d", k, m)), device(z, core, other)).wait_recv()

    for b in range(2):
        for j in range(3):
            sem(("g", b, j))
    for k in range(3):
        sem(("r", k))
        for m in range(1, TP):
            sem(("d", k, m))

    @pl.when(outer)
    def _():
        for copy in outer_sends():
            copy.start()
        for k in (0, 1, 2):
            rows_back(k).wait_recv()
            for m in range(1, TP):
                deliver(k, m, back_rows.at[k]).start()
            out_rows[k, mine, :] = back_rows[k]
        for copy in outer_sends():
            copy.wait_send()
        for b in range(2):
            for j in range(3):
                grad_back(b, j).wait_recv()
        for k in range(3):
            for m in range(1, TP):
                deliver(k, m, back_rows.at[k]).wait_send()
                deliver_wait(k, m)

    @pl.when(inner)
    def _():
        for copy in inner_sends():
            copy.start()
        peer_dev = device(z, peer, t)

        def shard_local(b):
            return local(shards[b], weights.at[b, 0], b)

        w_base = []
        for b in range(2):
            w_base.append(sem(("p", b, 0)))
            for s in range(1, 4):
                sem(("p", b, s))

        def shard_forward(b, s, src):
            return remote(src, weights.at[b, 4 + s], w_base[b] + s, peer_dev)

        def row_locals(a):
            src = (mid_in, cot_in, early_in, late_in)[a]
            out = []
            for m in range(TP):
                dst = late.at[0, m, pl.ds(0, q)] if a == 3 else acts.at[a, m, pl.ds(0, q)]
                out.append(local(src.at[own_quarter(column(m))], dst, 2 + TP * a + m))
            return out

        for b in range(2):
            shard_local(b).start()
            shard_forward(b, 0, shards[b]).start()
        for a in range(4):
            for copy in row_locals(a):
                copy.start()

        def spread_rows(a):
            src = (acts.at[a, 0], late.at[0, 0])[a == 3].at[pl.ds(q, q if a == 3 else 3 * q)]
            out = []
            for m in range(1, TP):
                full = late.at[0, m] if a == 3 else acts.at[a, m]
                dst = full.at[pl.ds(q, q if a == 3 else 3 * q)]
                out.append(remote(src, dst, sem(("s", a, m)), device(z, core, column(m))))
            return out

        def z_arrived(index, s):
            item = z_items[index]
            remote(item[2](s), item[2](s), z_base[item[0]] + s, mid_target).wait_recv()

        def gather_rows(a, index):
            for s in (1,) if a == 3 else (1, 2, 3):
                z_arrived(index, s)
            for copy in spread_rows(a):
                copy.start()

        def rows_ready(a):
            for copy in row_locals(a):
                copy.wait()
            for copy in spread_rows(a):
                copy.wait_recv()

        gather_rows(0, 0)
        gather_rows(1, 1)

        def normalize_block(b):
            @pl.loop(0, TP * PLANES)
            def _(i):
                at = pl.ds(pl.multiple_of((i % PLANES) * q, q), q)
                wide, factor = norm_parts(acts[2 * b, i // PLANES, at, :])
                normed[i // PLANES, at, :] = (wide * factor * gains[b][...]).astype(jnp.bfloat16)

        def rows_of(ref, h, cols):
            at = pl.ds(pl.multiple_of(h * half, half), half)
            return ref[:, at, cols].reshape(tile, width)

        def pre_block(b):
            acc[...] = jnp.zeros_like(acc)

            @pl.loop(0, 8)
            def _(i):
                slot, other = i // 2, i % 2

                @pl.when(i == 0)
                def _():
                    shard_local(b).wait()

                @pl.when((i > 0) & (other == 0))
                def _():
                    ref = weights.at[b, slot]
                    remote(ref, ref, z_base["w%d" % b] + slot, mid_target).wait_recv()
                    shard_forward(b, slot, ref).start()

                @pl.when(other == 1)
                def _():
                    ref = weights.at[b, 4 + slot]
                    remote(ref, ref, w_base[b] + slot, peer_dev).wait_recv()

                at = slot + 4 * other
                cols = feature(slot, other)

                @pl.loop(0, 2)
                def _(h):
                    piece = rows_of(normed, h, cols)
                    for j in range(2):
                        w = weights[b, at, pl.ds(j * hidden, hidden), :]
                        acc[j, h] += mm(piece, w, NT)

        def pieces_block(b):
            cots = acts.at[2 * b + 1]

            @pl.loop(0, 2)
            def _(h):
                late_acc[0] = jnp.zeros_like(late_acc[0])

                @pl.loop(0, 8)
                def _(i):
                    cols = feature(i % 4, i // 4)
                    w = weights[b, i, pl.ds(2 * hidden, hidden), :]
                    late_acc[0] += mm(rows_of(cots, h, cols), w, NT)

                @pl.loop(0, TP)
                def _(m):
                    at = pl.ds(pl.multiple_of(m * half, half), half)
                    to = pl.ds(pl.multiple_of(h * half, half), half)
                    gate, up = acc[0, h, at, :], acc[1, h, at, :]
                    grad = 0.5 * late_acc[0, at, :]
                    sig = 1.0 / (1.0 + jnp.exp(-gate))
                    act = gate * sig
                    turn = sig * (1.0 + gate * (1.0 - sig))
                    pieces[0, m, to, :] = (grad * up * turn).astype(jnp.bfloat16)
                    pieces[1, m, to, :] = (grad * act).astype(jnp.bfloat16)
                    pieces[2, m, to, :] = (act * up).astype(jnp.bfloat16)

        def swaps(b):
            out = []
            for j in range(3):
                out.append(remote(pieces.at[j], pieces_in.at[j], sem(("x", b, j)), peer_dev))
            for k in range(2):
                cols = feature(k, 1)
                for j, src in enumerate((normed, acts.at[2 * b + 1])):
                    out.append(
                        remote(src.at[:, :, cols], cols_in.at[j, k], sem(("y", b, j, k)), peer_dev)
                    )
            return out

        def part_copy(b, h, m, base):
            at = pl.ds(pl.multiple_of(h * half, half), half)
            dst = (part_in2, part_in1)[b]
            return remote(
                part.at[m, at], dst.at[m - 1, at], base + h * 3 + (m - 1),
                device(z, core, column(m)),
            )

        part_base = []
        for b in range(2):
            part_base.append(sem(("n", b, 0)))
            for i in range(1, 6):
                sem(("n", b, i))

        def grad_part(b):
            @pl.loop(0, 2 - b)
            def _(h):
                at = pl.ds(pl.multiple_of(h * half, half), half)

                @pl.loop(0, 8)
                def _(i):
                    cols = feature(i % 4, i // 4)
                    total = None
                    for j in range(2):
                        left = pieces[j, :, at, :].reshape(tile, hidden)
                        w = weights[b, i, pl.ds(j * hidden, hidden), :]
                        one = mm(left, w, NN)
                        total = one if j == 0 else total + one
                    part[:, at, cols] = total.astype(jnp.bfloat16).reshape(TP, half, width)

                for m in range(1, TP):
                    part_copy(b, h, m, part_base[b]).start()

        def fold(b):
            for copy in swaps(b):
                copy.wait_recv()
            tokens = TP * rows
            cots = acts.at[2 * b + 1]
            for k in range(2):
                cols = feature(k, 0)
                outs = grads[b] if k == 0 else sent[3 * b : 3 * b + 3]
                a0 = normed[:, :, cols].reshape(tokens, width)
                a1 = cols_in[0, k].reshape(tokens, width)
                for j in range(2):
                    one = mm(a0, pieces[j].reshape(tokens, hidden), TN)
                    one = one + mm(a1, pieces_in[j].reshape(tokens, hidden), TN)
                    outs[j][...] = one.astype(jnp.bfloat16)
                one = mm(pieces[2].reshape(tokens, hidden), cots[:, :, cols].reshape(tokens, width), TN)
                one = one + mm(
                    pieces_in[2].reshape(tokens, hidden), cols_in[1, k].reshape(tokens, width), TN
                )
                outs[2][...] = (0.5 * one).astype(jnp.bfloat16)
            for j in range(3):
                grad_back(b, j).start()

        def rows_grad(b, h, store):
            arrived = (part_in2, part_in1)[b]

            @pl.loop(0, 2)
            def _(i):
                at = pl.ds(pl.multiple_of(h * half + i * q, q), q)
                total = part[0, at, :].astype(jnp.float32)
                for m in range(1, TP):
                    total = total + arrived[m - 1, at, :].astype(jnp.float32)
                wide, factor = norm_parts(acts[2 * b, 0, at, :])
                scaled = total * gains[b][...]
                unit = wide * factor
                inner_mean = jnp.mean(scaled * unit, axis=-1, keepdims=True)
                cot = acts[2 * b + 1, 0, at, :].astype(jnp.float32)
                store(at, (cot + factor * (scaled - unit * inner_mean)).astype(jnp.bfloat16))

        def mid_copy(h, m, base):
            at = pl.ds(pl.multiple_of(h * half, half), half)
            return remote(
                acts.at[3, 0, at], acts.at[3, m, at], base + h * 3 + (m - 1),
                device(z, core, column(m)),
            )

        mid_base = sem(("a", 0))
        for i in range(1, 6):
            sem(("a", i))

        def late_block(b, n):
            @pl.loop(0, TP * 2)
            def _(i):
                at = pl.ds(pl.multiple_of((i % 2) * q, q), q)
                wide, factor = norm_parts(late[n, i // 2, at, :])
                late_normed[i // 2, at, :] = (wide * factor * gains[b][...]).astype(jnp.bfloat16)

            late_acc[...] = jnp.zeros_like(late_acc)

            @pl.loop(0, 8)
            def _(i):
                cols = feature(i % 4, i // 4)
                piece = late_normed[:, :, cols].reshape(tile, width)
                for j in range(2):
                    w = weights[b, i, pl.ds(j * hidden, hidden), :]
                    late_acc[j] += mm(piece, w, NT)

            gate = late_acc[0]
            hid = (gate / (1.0 + jnp.exp(-gate)) * late_acc[1]).astype(jnp.bfloat16)
            late_hid[...] = hid

            @pl.loop(0, 8)
            def _(i):
                cols = feature(i % 4, i // 4)
                w = weights[b, i, pl.ds(2 * hidden, hidden), :]
                one = mm(late_hid[...], w, NN).astype(jnp.bfloat16)
                late_part[:, :, cols] = one.reshape(TP, half, width)

            for m in range(1, TP):
                late_copy(n, m).start()

        def late_copy(n, m):
            return remote(
                late_part.at[m], late_part_in.at[n, m - 1], sem(("h", n, m)),
                device(z, core, column(m)),
            )

        def late_sum(n, store):
            for m in range(1, TP):
                late_copy(n, m).wait_recv()

            @pl.loop(0, 2)
            def _(i):
                at = pl.ds(pl.multiple_of(i * q, q), q)
                total = late_part[0, at, :].astype(jnp.float32)
                for m in range(1, TP):
                    total = total + late_part_in[n, m - 1, at, :].astype(jnp.float32)
                value = late[n, 0, at, :].astype(jnp.float32) + 0.5 * total
                store(at, value.astype(jnp.bfloat16))

        def late_spread(m):
            return remote(
                late.at[1, 0], late.at[1, m], sem(("k", m)), device(z, core, column(m))
            )

        rows_ready(0)
        normalize_block(0)
        pre_block(0)
        rows_ready(1)
        pieces_block(0)
        for copy in swaps(0):
            copy.start()
        grad_part(0)
        gather_rows(2, 3)
        gather_rows(3, 4)
        fold(0)

        def keep_mid(at, value):
            acts[3, 0, at, :] = value

        for h in range(2):
            for m in range(1, TP):
                part_copy(0, h, m, part_base[0]).wait_recv()
            rows_grad(0, h, keep_mid)
            for m in range(1, TP):
                mid_copy(h, m, mid_base).start()
        for copy in swaps(0):
            copy.wait_send()
        pl.semaphore_signal(ack, inc=1, device_id=peer_dev, device_id_type=pl.DeviceIdType.MESH)

        rows_ready(2)
        normalize_block(1)
        pre_block(1)
        rows_ready(3)
        late_block(1, 0)
        for h in range(2):
            for m in range(1, TP):
                mid_copy(h, m, mid_base).wait_recv()
        pieces_block(1)
        pl.semaphore_wait(ack, 1)
        for copy in swaps(1):
            copy.start()
        for h in range(2):
            for m in range(1, TP):
                part_copy(0, h, m, part_base[0]).wait_send()
        grad_part(1)

        def keep_late(at, value):
            late[1, 0, at, :] = value

        late_sum(0, keep_late)
        for m in range(1, TP):
            late_spread(m).start()
        rows_back(0).start()
        fold(1)
        for m in range(1, TP):
            late_spread(m).wait_recv()
            late_copy(0, m).wait_send()
        late_block(0, 1)
        for m in range(1, TP):
            part_copy(1, 0, m, part_base[1]).wait_recv()

        def keep_done(index):
            def store(at, value):
                done_rows[index, at, :] = value

            return store

        rows_grad(1, 0, keep_done(1))
        rows_back(2).start()
        late_sum(1, keep_done(0))
        rows_back(1).start()
        for k in range(3):
            src = row_source(k).at[pl.ds(0, q)]
            for m in range(1, TP):
                deliver(k, m, src).start()
            out_rows[k, mine, :] = src[...]

        for copy in inner_sends():
            copy.wait_send()
        for b in range(2):
            for s in range(4):
                src = shards[b] if s == 0 else weights.at[b, s]
                shard_forward(b, s, src).wait_send()
            for j in range(3):
                grad_back(b, j).wait_send()
        for a in range(4):
            for copy in spread_rows(a):
                copy.wait_send()
        for copy in swaps(1):
            copy.wait_send()
        for m in range(1, TP):
            for h in range(2):
                mid_copy(h, m, mid_base).wait_send()
            part_copy(1, 0, m, part_base[1]).wait_send()
            late_spread(m).wait_send()
            late_copy(1, m).wait_send()
        for k in range(3):
            rows_back(k).wait_send()
            for m in range(1, TP):
                deliver(k, m, row_source(k).at[pl.ds(0, q)]).wait_send()
                deliver_wait(k, m)


def per_device(
    late_input,
    early_input,
    early_mid,
    cotangent,
    gain_first,
    gain_second,
    gate_first,
    up_first,
    down_first,
    gate_second,
    up_second,
    down_second,
    *sums,
):
    count, feats = late_input.shape
    width, hidden = gate_first.shape
    q = count // TP
    half = 2 * q
    tile = TP * half
    bf = jnp.bfloat16
    shard_second = jnp.concatenate((gate_second.T, up_second.T, down_second), axis=0)
    shard_first = jnp.concatenate((gate_first.T, up_first.T, down_first), axis=0)
    wide, tall = (width, hidden), (hidden, width)
    grad_shapes = [wide, wide, tall] * 2
    anywhere = pl.BlockSpec(memory_space=pl.ANY)
    in_vmem = pl.BlockSpec(memory_space=pltpu.VMEM)
    outs = pl.pallas_call(
        step_kernel,
        out_shape=[jax.ShapeDtypeStruct((3, count, feats), bf)]
        + [jax.ShapeDtypeStruct(s, bf) for s in grad_shapes],
        in_specs=[anywhere] * 4 + [in_vmem] * 2 + [anywhere] * 2,
        out_specs=[in_vmem] * 7,
        scratch_shapes=[
            pltpu.VMEM((2, 8, 3 * hidden, width), bf),
            pltpu.VMEM((4, TP, count, feats), bf),
            pltpu.VMEM((2, TP, half, feats), bf),
            pltpu.VMEM((TP, count, feats), bf),
            pltpu.VMEM((TP, half, feats), bf),
            pltpu.VMEM((3, TP, count, hidden), bf),
            pltpu.VMEM((3, TP, count, hidden), bf),
            pltpu.VMEM((2, 2, TP, count, width), bf),
            pltpu.VMEM((TP, count, feats), bf),
            pltpu.VMEM((3, count, feats), bf),
            pltpu.VMEM((3, half, feats), bf),
            pltpu.VMEM((TP, half, feats), bf),
            pltpu.VMEM((2, 3, half, feats), bf),
            [pltpu.VMEM(s, bf) for s in grad_shapes],
            pltpu.VMEM((3, q, feats), bf),
            pltpu.VMEM((2, half, feats), bf),
            pltpu.VMEM((2, 2, tile, hidden), jnp.float32),
            pltpu.VMEM((2, tile, hidden), jnp.float32),
            pltpu.VMEM((tile, hidden), bf),
            pltpu.SemaphoreType.DMA((128,)),
            pltpu.SemaphoreType.DMA((128,)),
            pltpu.SemaphoreType.DMA((18,)),
            pltpu.SemaphoreType.REGULAR,
        ],
        compiler_params=pltpu.CompilerParams(
            collective_id=0, has_side_effects=True, vmem_limit_bytes=67043328
        ),
        name="step",
    )(
        late_input, early_mid, cotangent, early_input,
        gain_second.reshape((1, -1)), gain_first.reshape((1, -1)),
        shard_second, shard_first,
    )
    rows, second, first = outs[0], outs[1:4], outs[4:7]
    grads = tuple(first) + tuple(second)
    return (rows[0], rows[1], rows[2]) + tuple(
        old + new.astype(jnp.float32) for old, new in zip(sums, grads)
    )


def normalize(values, gain_vector):
    widened = values.astype(jnp.float32)
    factor = lax.rsqrt(jnp.mean(widened * widened, axis=-1, keepdims=True) + norm_eps)
    normed = (widened * factor * gain_vector).astype(jnp.bfloat16)
    return (widened, factor, normed)


def project(rows, weights):
    return jnp.dot(rows, weights, preferred_element_type=jnp.float32)


def project_back(hidden_rows, weights):
    return jnp.einsum("tf,df->td", hidden_rows, weights, preferred_element_type=jnp.float32)


def fold_rows(left, right):
    return jnp.einsum("ta,tb->ab", left, right, preferred_element_type=jnp.float32)


def own_rows(rows):
    count = rows.shape[0] // lax.axis_size("tp")
    return lax.dynamic_slice_in_dim(rows, lax.axis_index("tp") * count, count, axis=0)


def sum_rows(partial):
    shares = lax.all_to_all(
        partial.astype(jnp.bfloat16), "tp", split_axis=0, concat_axis=0, tiled=True
    )
    shares = shares.reshape((lax.axis_size("tp"), -1, shares.shape[1]))
    return jnp.sum(shares.astype(jnp.float32), axis=0)


def join_rows(rows):
    return lax.all_gather(rows, "tp", axis=0, tiled=True)


def block_forward(values, gain_vector, weights, width):
    widened, factor, normed = normalize(values, gain_vector)
    pre = project(normed, weights[:, : 2 * width])
    hidden = (jax.nn.silu(pre[:, :width]) * pre[:, width:]).astype(jnp.bfloat16)
    branch = sum_rows(project_back(hidden, weights[:, 2 * width :]))
    return join_rows((own_rows(widened) + 0.5 * branch).astype(jnp.bfloat16))


def block_backward(normalized, cotangent, weights, width):
    widened, factor, normed = normalized
    pre = project(normed, weights[:, : 2 * width])
    gate_pre, up_pre = pre[:, :width], pre[:, width:]
    sigmoid_gate = jax.nn.sigmoid(gate_pre)
    activated = gate_pre * sigmoid_gate
    hidden = (activated * up_pre).astype(jnp.bfloat16)
    hidden_grad = 0.5 * project(cotangent, weights[:, 2 * width :])
    gate_grad = (
        hidden_grad * up_pre * sigmoid_gate * (1.0 + gate_pre * (1.0 - sigmoid_gate))
    ).astype(jnp.bfloat16)
    up_grad = (hidden_grad * activated).astype(jnp.bfloat16)
    pieces = jnp.concatenate((gate_grad, up_grad, hidden), axis=1)
    partial_value = project_back(pieces[:, : 2 * width], weights[:, : 2 * width])
    return (partial_value, pieces)


def backward_rows(normalized, cotangent, gain_vector, partial_value):
    normed_grad = sum_rows(partial_value)
    widened, factor = own_rows(normalized[0]), own_rows(normalized[1])
    scaled = normed_grad * gain_vector
    unit_rows = widened * factor
    rows_grad = own_rows(cotangent).astype(jnp.float32) + factor * (
        scaled - unit_rows * jnp.mean(scaled * unit_rows, axis=-1, keepdims=True)
    )
    return rows_grad.astype(jnp.bfloat16)


def gather_weights(gate, up, down):
    return lax.all_gather(jnp.concatenate((gate, up, down.T), axis=1), "fs", axis=0, tiled=True)


def share_columns(rows):
    return lax.all_to_all(rows, "fs", split_axis=1, concat_axis=0, tiled=True)


def join_columns(share):
    joined = join_rows(share)
    parts = joined.reshape((lax.axis_size("tp"), lax.axis_size("fs"), -1, joined.shape[1]))
    return jnp.swapaxes(parts, 0, 1).reshape(joined.shape)


def per_device_general(
    late_input,
    early_input,
    early_mid,
    cotangent,
    gain_first,
    gain_second,
    gate_first,
    up_first,
    down_first,
    gate_second,
    up_second,
    down_second,
    sum_gate_first,
    sum_up_first,
    sum_down_first,
    sum_gate_second,
    sum_up_second,
    sum_down_second,
):
    width = gate_first.shape[1]
    weights_second = gather_weights(gate_second, up_second, down_second)
    weights_first = gather_weights(gate_first, up_first, down_first)
    norm_second = normalize(early_mid, gain_second)
    norm_first = normalize(early_input, gain_first)
    early_rows = jnp.stack(
        (own_rows(norm_second[2]), own_rows(norm_first[2]), own_rows(cotangent))
    )
    early_shares = lax.all_to_all(early_rows, "fs", split_axis=2, concat_axis=1, tiled=True)
    columns_second = join_columns(early_shares[0])
    columns_first = join_columns(early_shares[1])
    columns_cotangent = join_columns(early_shares[2])
    partial_second, pieces_second = block_backward(
        norm_second, cotangent, weights_second, width
    )
    all_second = lax.all_gather(pieces_second, "fs", axis=0, tiled=True)
    mid_rows = backward_rows(norm_second, cotangent, gain_second, partial_second)
    mid_grad = join_rows(mid_rows)
    columns_mid = join_columns(share_columns(mid_rows))
    partial_first, pieces_first = block_backward(norm_first, mid_grad, weights_first, width)
    all_first = lax.all_gather(pieces_first, "fs", axis=0, tiled=True)
    late_mid = block_forward(late_input, gain_first, weights_first, width)
    input_grad = join_rows(backward_rows(norm_first, mid_grad, gain_first, partial_first))
    late_out = block_forward(late_mid, gain_second, weights_second, width)

    def collect(pieces, columns_in, columns_out, sums):
        return (
            sums[0] + fold_rows(columns_in, pieces[:, :width]),
            sums[1] + fold_rows(columns_in, pieces[:, width : 2 * width]),
            sums[2] + 0.5 * fold_rows(pieces[:, 2 * width :], columns_out),
        )

    new_second = collect(
        all_second, columns_second, columns_cotangent, (sum_gate_second, sum_up_second, sum_down_second)
    )
    new_first = collect(
        all_first, columns_first, columns_mid, (sum_gate_first, sum_up_first, sum_down_first)
    )
    return (late_mid, late_out, input_grad) + new_first + new_second


def solution(mesh):
    rows, up_down, down_up = P("fs", None), P("fs", "tp"), P("tp", "fs")
    weights = (up_down, up_down, down_up)
    in_specs = (rows,) * 4 + (P(), P()) + weights * 4
    out_specs = (rows,) * 3 + weights * 2
    line_of_four = mesh.shape["fs"] == PLANES * CORES and mesh.shape["tp"] == TP
    body = per_device if line_of_four else per_device_general
    return jax.shard_map(
        body, mesh=mesh, in_specs=in_specs, out_specs=out_specs, check_vma=False
    )
```

```python
import functools

import jax
import jax.numpy as jnp
from jax import lax
from jax.experimental import pallas as pl
from jax.experimental.pallas import tpu as pltpu
from jax.sharding import PartitionSpec as P

norm_eps = 1e-06
CORES = 2
TP = 4
PLANES = 4

NT = (((1,), (1,)), ((), ()))
NN = (((1,), (0,)), ((), ()))
TN = (((0,), (0,)), ((), ()))


def mm(left, right, dims):
    return lax.dot_general(left, right, dims, preferred_element_type=jnp.float32)


def norm_parts(rows):
    wide = rows.astype(jnp.float32)
    factor = lax.rsqrt(jnp.mean(wide * wide, axis=-1, keepdims=True) + norm_eps)
    return wide, factor


def step_kernel(
    late_in, mid_in, cot_in, early_in, gain2, gain1,
    gate2, up2, down2, gate1, up1, down1,
    late_mid, late_out, grad_in, grads2, grads1,
    weights, acts, late, normed, late_normed, pieces, pieces_in, cols_in,
    part, part_in2, part_in1, late_part, late_part_in, sent, back_rows, done_rows,
    acc, late_acc, late_hid, send_sems, recv_sems, local_sems, ack,
):
    f, t = lax.axis_index("fs"), lax.axis_index("tp")
    z, core = f // CORES, f % CORES
    peer = 1 - core
    inner = (z == 1) | (z == 2)
    outer = (z == 0) | (z == 3)
    near, upper = (z // 2) * 3, z // 2
    q = late_in.shape[0] // TP
    rows = PLANES * q
    half = 2 * q
    hidden, width = down2.shape
    tile = TP * half
    grads = (grads2, grads1)
    shards = ((gate2, up2, down2), (gate1, up1, down1))
    out_rows = (late_mid, late_out, grad_in)
    gains = (gain2, gain1)
    ids = {}

    def sem(name):
        return ids.setdefault(name, len(ids))

    def column(mask):
        x, y = t % 2, t // 2
        gx, gy = mask % 2, mask // 2
        x = x + gx - 2 * x * gx
        y = y + gy - 2 * y * gy
        return y * 2 + x

    def device(zz, cc, tt):
        return (zz * CORES + cc, tt)

    def remote(src, dst, index, where):
        return pltpu.make_async_remote_copy(
            src_ref=src, dst_ref=dst, send_sem=send_sems.at[index],
            recv_sem=recv_sems.at[index], device_id=where,
            device_id_type=pl.DeviceIdType.MESH,
        )

    def local(src, dst, index):
        return pltpu.make_async_copy(src, dst, local_sems.at[index])

    def own_quarter(tt):
        return pl.ds(pl.multiple_of(tt * q, q), q)

    def feature(slot, other):
        v = slot + (1 - slot // 2) * (1 - 2 * slot)
        zs = v + upper * (3 - 2 * v)
        cc = core + other - 2 * core * other
        return pl.ds(pl.multiple_of((zs * CORES + cc) * width, width), width)

    barrier = pltpu.get_barrier_semaphore()
    friends = [device((z + k) % PLANES, core, t) for k in range(1, PLANES)]
    friends += [device(z, peer, t)] + [device(z, core, column(m)) for m in range(1, TP)]
    for friend in friends:
        pl.semaphore_signal(barrier, inc=1, device_id=friend, device_id_type=pl.DeviceIdType.MESH)
    pl.semaphore_wait(barrier, len(friends))

    mine = own_quarter(t)
    parts = [pl.ds(j * hidden, hidden) for j in range(3)]

    def row_item(name, ref, store):
        return (name, ref.at[mine], lambda s: store.at[pl.ds(s * q, q)])

    def shard_item(b, j):
        return (("w", b, j), shards[b][j], lambda s: weights.at[b, s, parts[j]])

    z_items = [row_item("m", mid_in, acts.at[0, 0]), row_item("c", cot_in, acts.at[1, 0])]
    z_items += [shard_item(0, 0), shard_item(0, 1)]
    z_items += [row_item("e", early_in, acts.at[2, 0]), row_item("l", late_in, late.at[0, 0])]
    z_items += [shard_item(0, 2)]
    z_items += [shard_item(1, j) for j in range(3)]
    z_base = {}
    for name, _, _ in z_items:
        z_base[name] = sem((name, 0))
        for s in range(1, 4):
            sem((name, s))

    def z_copy(item, s, where):
        name, src, to = item
        return remote(src, to(s), z_base[name] + s, where)

    first_target = device(1 + upper, core, t)
    second_target = device(2 - upper, core, t)
    mid_target = device(3 - z, core, t)

    def outer_sends():
        out = []
        for item in z_items:
            out.append(z_copy(item, 1, first_target))
            if item[0] != "l":
                out.append(z_copy(item, 3, second_target))
        return out

    def inner_sends():
        return [z_copy(item, 2, mid_target) for item in z_items if item[0] != "l"]

    out_dev = device(near, core, t)

    def grad_back(b, j):
        return remote(sent.at[b, j], grads[b].at[j], sem(("g", b, j)), out_dev)

    def row_source(k):
        return (late.at[1, 0], done_rows.at[0], done_rows.at[1])[k]

    def rows_back(k):
        return remote(row_source(k).at[pl.ds(q, q)], back_rows.at[k], sem(("r", k)), out_dev)

    def deliver(k, m, src):
        return remote(src, out_rows[k].at[mine], sem(("d", k, m)), device(z, core, column(m)))

    def deliver_wait(k, m):
        other = column(m)
        dst = out_rows[k].at[own_quarter(other)]
        remote(dst, dst, sem(("d", k, m)), device(z, core, other)).wait_recv()

    for b in range(2):
        for j in range(3):
            sem(("g", b, j))
    for k in range(3):
        sem(("r", k))
        for m in range(1, TP):
            sem(("d", k, m))

    @pl.when(outer)
    def _():
        for copy in outer_sends():
            copy.start()
        for k in (0, 2, 1):
            rows_back(k).wait_recv()
            for m in range(1, TP):
                deliver(k, m, back_rows.at[k]).start()
            out_rows[k][mine, :] = back_rows[k]
        for copy in outer_sends():
            copy.wait_send()
        for b in range(2):
            for j in range(3):
                grad_back(b, j).wait_recv()
        for k in range(3):
            for m in range(1, TP):
                deliver(k, m, back_rows.at[k]).wait_send()
                deliver_wait(k, m)

    @pl.when(inner)
    def _():
        for copy in inner_sends():
            copy.start()
        peer_dev = device(z, peer, t)

        def shard_local(b, j):
            return local(shards[b][j], weights.at[b, 0, parts[j]], 3 * b + j)

        w_base = []
        for b in range(2):
            w_base.append([])
            for j in range(3):
                w_base[b].append(sem(("p", b, j, 0)))
                for s in range(1, 4):
                    sem(("p", b, j, s))

        def shard_forward(b, j, s, src):
            return remote(src, weights.at[b, 4 + s, parts[j]], w_base[b][j] + s, peer_dev)

        def row_locals(a):
            src = (mid_in, cot_in, early_in, late_in)[a]
            out = []
            for m in range(TP):
                dst = late.at[0, m, pl.ds(0, q)] if a == 3 else acts.at[a, m, pl.ds(0, q)]
                out.append(local(src.at[own_quarter(column(m))], dst, 6 + TP * a + m))
            return out

        for a in range(4):
            for copy in row_locals(a):
                copy.start()
        for b in range(2):
            for j in range(3):
                shard_local(b, j).start()
                shard_forward(b, j, 0, shards[b][j]).start()

        def spread_rows(a):
            src = (acts.at[a, 0], late.at[0, 0])[a == 3].at[pl.ds(q, q if a == 3 else 3 * q)]
            out = []
            for m in range(1, TP):
                full = late.at[0, m] if a == 3 else acts.at[a, m]
                dst = full.at[pl.ds(q, q if a == 3 else 3 * q)]
                out.append(remote(src, dst, sem(("s", a, m)), device(z, core, column(m))))
            return out

        def z_arrived(index, s):
            item = z_items[index]
            remote(item[2](s), item[2](s), z_base[item[0]] + s, mid_target).wait_recv()

        def gather_rows(a, index):
            for s in (1,) if a == 3 else (1, 2, 3):
                z_arrived(index, s)
            for copy in spread_rows(a):
                copy.start()

        def rows_ready(a):
            for copy in row_locals(a):
                copy.wait()
            for copy in spread_rows(a):
                copy.wait_recv()

        gather_rows(0, 0)
        gather_rows(1, 1)

        def normalize_block(b):
            @pl.loop(0, TP * PLANES)
            def _(i):
                at = pl.ds(pl.multiple_of((i % PLANES) * q, q), q)
                wide, factor = norm_parts(acts[2 * b, i // PLANES, at, :])
                normed[i // PLANES, at, :] = (wide * factor * gains[b][...]).astype(jnp.bfloat16)

        def rows_of(ref, h, cols):
            at = pl.ds(pl.multiple_of(h * half, half), half)
            return ref[:, at, cols].reshape(tile, width)

        def take_part(b, j, slot, other):
            @pl.when((slot == 0) & (other == 0))
            def _():
                shard_local(b, j).wait()

            @pl.when((slot > 0) & (other == 0))
            def _():
                ref = weights.at[b, slot, parts[j]]
                remote(ref, ref, z_base[("w", b, j)] + slot, mid_target).wait_recv()
                shard_forward(b, j, slot, ref).start()

            @pl.when(other == 1)
            def _():
                ref = weights.at[b, 4 + slot, parts[j]]
                remote(ref, ref, w_base[b][j] + slot, peer_dev).wait_recv()

        def pre_block(b):
            acc[...] = jnp.zeros_like(acc)

            @pl.loop(0, 8)
            def _(i):
                slot, other = i // 2, i % 2
                for j in range(2):
                    take_part(b, j, slot, other)
                at = slot + 4 * other
                cols = feature(slot, other)

                @pl.loop(0, 2)
                def _(h):
                    piece = rows_of(normed, h, cols)
                    for j in range(2):
                        acc[j, h] += mm(piece, weights[b, at, parts[j], :], NT)

        def take_down(b):
            @pl.loop(0, 8)
            def _(i):
                take_part(b, 2, i // 2, i % 2)

        def down_block(b, take):
            cots = acts.at[2 * b + 1]
            late_acc[...] = jnp.zeros_like(late_acc)

            @pl.loop(0, 8)
            def _(i):
                slot, other = i // 2, i % 2
                if take:
                    take_part(b, 2, slot, other)
                cols = feature(slot, other)

                @pl.loop(0, 2)
                def _(h):
                    w = weights[b, slot + 4 * other, parts[2], :]
                    late_acc[h] += mm(rows_of(cots, h, cols), w, NT)

        def pieces_block(h):
            @pl.loop(0, TP)
            def _(m):
                at = pl.ds(pl.multiple_of(m * half, half), half)
                to = pl.ds(pl.multiple_of(h * half, half), half)
                gate, up = acc[0, h, at, :], acc[1, h, at, :]
                grad = 0.5 * late_acc[h, at, :]
                sig = 1.0 / (1.0 + jnp.exp(-gate))
                act = gate * sig
                turn = sig * (1.0 + gate * (1.0 - sig))
                pieces[0, m, to, :] = (grad * up * turn).astype(jnp.bfloat16)
                pieces[1, m, to, :] = (grad * act).astype(jnp.bfloat16)
                pieces[2, m, to, :] = (act * up).astype(jnp.bfloat16)

        def swaps(b):
            out = []
            for j in range(3):
                out.append(remote(pieces.at[j], pieces_in.at[j], sem(("x", b, j)), peer_dev))
            for k in range(2):
                cols = feature(k, 1)
                for j, src in enumerate((normed, acts.at[2 * b + 1])):
                    out.append(
                        remote(src.at[:, :, cols], cols_in.at[j, k], sem(("y", b, j, k)), peer_dev)
                    )
            return out

        def part_rows(b, r):
            size = half if b == 0 else q
            return pl.ds(r * size, size)

        def part_copy(b, r, m):
            at = part_rows(b, r)
            return remote(
                part.at[m, at], (part_in2, part_in1)[b].at[m - 1, at], sem(("n", b, r, m)),
                device(z, core, column(m)),
            )

        def grad_part(b, h):
            at = pl.ds(h * half, half)

            @pl.loop(0, 8)
            def _(i):
                cols = feature(i % 4, i // 4)
                total = None
                for j in range(2):
                    left = pieces[j, :, at, :].reshape(tile, hidden)
                    one = mm(left, weights[b, i, parts[j], :], NN)
                    total = one if j == 0 else total + one
                part[:, at, cols] = total.astype(jnp.bfloat16).reshape(TP, half, width)

        def fold(b):
            for copy in swaps(b):
                copy.wait_recv()
            tokens = TP * rows
            cots = acts.at[2 * b + 1]
            for k in (1, 0):
                cols = feature(k, 0)
                out = sent.at[b] if k == 1 else grads[b]
                sides = (
                    (normed[:, :, cols].reshape(tokens, width), cols_in[0, k].reshape(tokens, width)),
                    (cots[:, :, cols].reshape(tokens, width), cols_in[1, k].reshape(tokens, width)),
                )
                for j in range(3):
                    own, other = sides[j // 2]
                    one = mm(pieces[j].reshape(tokens, hidden), own, TN)
                    one = one + mm(pieces_in[j].reshape(tokens, hidden), other, TN)
                    out[j] = (one if j < 2 else 0.5 * one).astype(jnp.bfloat16)
                    if k == 1 and (b == 0 or j < 2):
                        grad_back(b, j).start()

        def rows_grad(b, r, out):
            for m in range(1, TP):
                part_copy(b, r, m).wait_recv()
            arrived = (part_in2, part_in1)[b]
            at = part_rows(b, r)
            total = part[0, at, :].astype(jnp.float32)
            for m in range(1, TP):
                total = total + arrived[m - 1, at, :].astype(jnp.float32)
            wide, factor = norm_parts(acts[2 * b, 0, at, :])
            scaled = total * gains[b][...]
            unit = wide * factor
            inner_mean = jnp.mean(scaled * unit, axis=-1, keepdims=True)
            cot = acts[2 * b + 1, 0, at, :].astype(jnp.float32)
            out[at, :] = (cot + factor * (scaled - unit * inner_mean)).astype(jnp.bfloat16)

        def mid_copy(h, m):
            at = pl.ds(h * half, half)
            return remote(
                acts.at[3, 0, at], acts.at[3, m, at], sem(("a", h, m)),
                device(z, core, column(m)),
            )

        def late_block(b, n, take):
            @pl.loop(0, TP * 2)
            def _(i):
                at = pl.ds(pl.multiple_of((i % 2) * q, q), q)
                wide, factor = norm_parts(late[n, i // 2, at, :])
                late_normed[i // 2, at, :] = (wide * factor * gains[b][...]).astype(jnp.bfloat16)

            late_acc[...] = jnp.zeros_like(late_acc)

            @pl.loop(0, 8)
            def _(i):
                cols = feature(i % 4, i // 4)
                piece = late_normed[:, :, cols].reshape(tile, width)
                for j in range(2):
                    late_acc[j] += mm(piece, weights[b, i, parts[j], :], NT)

            gate = late_acc[0]
            hid = (gate / (1.0 + jnp.exp(-gate)) * late_acc[1]).astype(jnp.bfloat16)
            late_hid[...] = hid
            if take:
                take_down(b)

            @pl.loop(0, 8)
            def _(i):
                cols = feature(i % 4, i // 4)
                one = mm(late_hid[...], weights[b, i, parts[2], :], NN).astype(jnp.bfloat16)
                late_part[:, :, cols] = one.reshape(TP, half, width)

            for r in (1, 0):
                for m in range(1, TP):
                    late_copy(n, r, m).start()

        def late_copy(n, r, m):
            at = pl.ds(r * q, q)
            return remote(
                late_part.at[m, at], late_part_in.at[n, m - 1, at], sem(("h", n, r, m)),
                device(z, core, column(m)),
            )

        def late_sum(n, r, out):
            for m in range(1, TP):
                late_copy(n, r, m).wait_recv()
            at = pl.ds(r * q, q)
            total = late_part[0, at, :].astype(jnp.float32)
            for m in range(1, TP):
                total = total + late_part_in[n, m - 1, at, :].astype(jnp.float32)
            value = late[n, 0, at, :].astype(jnp.float32) + 0.5 * total
            out[at, :] = value.astype(jnp.bfloat16)

        def late_spread(m):
            return remote(
                late.at[1, 0], late.at[1, m], sem(("k", m)), device(z, core, column(m))
            )

        rows_ready(0)
        normalize_block(0)
        pre_block(0)
        rows_ready(1)
        gather_rows(2, 4)
        gather_rows(3, 5)
        down_block(0, True)
        for h in range(2):
            pieces_block(h)
            grad_part(0, h)
            for m in range(1, TP):
                part_copy(0, h, m).start()
        for copy in swaps(0):
            copy.start()
        for h in range(2):
            rows_grad(0, h, acts.at[3, 0])
            for m in range(1, TP):
                mid_copy(h, m).start()
            if h == 0:
                fold(0)
        for copy in swaps(0):
            copy.wait_send()
        pl.semaphore_signal(ack, inc=1, device_id=peer_dev, device_id_type=pl.DeviceIdType.MESH)

        rows_ready(2)
        normalize_block(1)
        pre_block(1)
        rows_ready(3)
        late_block(1, 0, True)
        for h in range(2):
            for m in range(1, TP):
                mid_copy(h, m).wait_recv()
        down_block(1, False)

        @pl.loop(0, 2)
        def _(h):
            pieces_block(h)

        pl.semaphore_wait(ack, 1)
        for copy in swaps(1):
            copy.start()
        for r in range(2):
            for m in range(1, TP):
                part_copy(0, r, m).wait_send()
        grad_part(1, 0)
        late_rows = late.at[1, 0]
        late_sum(0, 1, late_rows)
        late_sum(0, 0, late_rows)
        for m in range(1, TP):
            late_spread(m).start()
        rows_back(0).start()
        for r in (1, 0):
            for m in range(1, TP):
                part_copy(1, r, m).start()
        fold(1)
        for m in range(1, TP):
            late_spread(m).wait_recv()
            for r in range(2):
                late_copy(0, r, m).wait_send()
        late_block(0, 1, False)
        for m in range(TP):
            late_mid[own_quarter(column(m)), :] = late[1, m, pl.ds(0, q), :]

        def finish(k):
            src = row_source(k).at[pl.ds(0, q)]
            for m in range(1, TP):
                deliver(k, m, src).start()
            out_rows[k][mine, :] = src[...]

        rows_grad(1, 1, done_rows.at[1])
        rows_back(2).start()
        rows_grad(1, 0, done_rows.at[1])
        late_sum(1, 1, done_rows.at[0])
        rows_back(1).start()
        grad_back(1, 2).start()
        finish(2)
        late_sum(1, 0, done_rows.at[0])
        finish(1)

        for copy in inner_sends():
            copy.wait_send()
        for b in range(2):
            for j in range(3):
                for s in range(4):
                    src = shards[b][j] if s == 0 else weights.at[b, s, parts[j]]
                    shard_forward(b, j, s, src).wait_send()
                grad_back(b, j).wait_send()
        for a in range(4):
            for copy in spread_rows(a):
                copy.wait_send()
        for copy in swaps(1):
            copy.wait_send()
        for m in range(1, TP):
            for r in range(2):
                mid_copy(r, m).wait_send()
                part_copy(1, r, m).wait_send()
                late_copy(1, r, m).wait_send()
            late_spread(m).wait_send()
        for k in range(3):
            rows_back(k).wait_send()
            if k > 0:
                for m in range(1, TP):
                    deliver(k, m, row_source(k).at[pl.ds(0, q)]).wait_send()
                    deliver_wait(k, m)


def add_kernel(r0, r1, r2, grads2, grads1, *refs):
    olds, outs = refs[:6], refs[6:]
    for src, dst in zip((r0, r1, r2), outs[:3]):
        dst[...] = src[...]
    for j in range(6):
        grads = (grads1, grads2)[j // 3]
        outs[3 + j][...] = olds[j][...] + grads[j % 3].astype(jnp.float32)


def per_device(
    late_input,
    early_input,
    early_mid,
    cotangent,
    gain_first,
    gain_second,
    gate_first,
    up_first,
    down_first,
    gate_second,
    up_second,
    down_second,
    *sums,
):
    count, feats = late_input.shape
    width, hidden = gate_first.shape
    q = count // TP
    half = 2 * q
    tile = TP * half
    bf = jnp.bfloat16
    anywhere = pl.BlockSpec(memory_space=pl.ANY)
    in_vmem = pl.BlockSpec(memory_space=pltpu.VMEM)
    rows_shape = jax.ShapeDtypeStruct((count, feats), bf)
    grads_shape = jax.ShapeDtypeStruct((3, hidden, width), bf)
    outs = pl.pallas_call(
        step_kernel,
        out_shape=[rows_shape] * 3 + [grads_shape] * 2,
        in_specs=[anywhere] * 4 + [in_vmem] * 2 + [anywhere] * 6,
        out_specs=[in_vmem] * 5,
        scratch_shapes=[
            pltpu.VMEM((2, 8, 3 * hidden, width), bf),
            pltpu.VMEM((4, TP, count, feats), bf),
            pltpu.VMEM((2, TP, half, feats), bf),
            pltpu.VMEM((TP, count, feats), bf),
            pltpu.VMEM((TP, half, feats), bf),
            pltpu.VMEM((3, TP, count, hidden), bf),
            pltpu.VMEM((3, TP, count, hidden), bf),
            pltpu.VMEM((2, 2, TP, count, width), bf),
            pltpu.VMEM((TP, count, feats), bf),
            pltpu.VMEM((3, count, feats), bf),
            pltpu.VMEM((3, half, feats), bf),
            pltpu.VMEM((TP, half, feats), bf),
            pltpu.VMEM((2, 3, half, feats), bf),
            pltpu.VMEM((2, 3, hidden, width), bf),
            pltpu.VMEM((3, q, feats), bf),
            pltpu.VMEM((2, half, feats), bf),
            pltpu.VMEM((2, 2, tile, hidden), jnp.float32),
            pltpu.VMEM((2, tile, hidden), jnp.float32),
            pltpu.VMEM((tile, hidden), bf),
            pltpu.SemaphoreType.DMA((160,)),
            pltpu.SemaphoreType.DMA((160,)),
            pltpu.SemaphoreType.DMA((22,)),
            pltpu.SemaphoreType.REGULAR,
        ],
        compiler_params=pltpu.CompilerParams(
            collective_id=0, has_side_effects=True, vmem_limit_bytes=67043328
        ),
        name="step",
    )(
        late_input, early_mid, cotangent, early_input,
        gain_second.reshape((1, -1)), gain_first.reshape((1, -1)),
        gate_second.T, up_second.T, down_second,
        gate_first.T, up_first.T, down_first,
    )
    tall = [old.T if j % 3 < 2 else old for j, old in enumerate(sums)]
    steps = 4
    row_spec = pl.BlockSpec((count // steps, feats), lambda i: (i, 0))
    sum_spec = pl.BlockSpec((hidden // steps, width), lambda i: (i, 0))
    grad_spec = pl.BlockSpec((3, hidden // steps, width), lambda i: (0, i, 0))
    done = pl.pallas_call(
        add_kernel,
        grid=(steps,),
        out_shape=[rows_shape] * 3 + [jax.ShapeDtypeStruct((hidden, width), jnp.float32)] * 6,
        in_specs=[row_spec] * 3 + [grad_spec] * 2 + [sum_spec] * 6,
        out_specs=[row_spec] * 3 + [sum_spec] * 6,
        name="add",
    )(*outs, *tall)
    fresh = [new.T if j % 3 < 2 else new for j, new in enumerate(done[3:])]
    return tuple(done[:3]) + tuple(fresh)


def normalize(values, gain_vector):
    widened = values.astype(jnp.float32)
    factor = lax.rsqrt(jnp.mean(widened * widened, axis=-1, keepdims=True) + norm_eps)
    normed = (widened * factor * gain_vector).astype(jnp.bfloat16)
    return (widened, factor, normed)


def project(rows, weights):
    return jnp.dot(rows, weights, preferred_element_type=jnp.float32)


def project_back(hidden_rows, weights):
    return jnp.einsum("tf,df->td", hidden_rows, weights, preferred_element_type=jnp.float32)


def fold_rows(left, right):
    return jnp.einsum("ta,tb->ab", left, right, preferred_element_type=jnp.float32)


def own_rows(rows):
    count = rows.shape[0] // lax.axis_size("tp")
    return lax.dynamic_slice_in_dim(rows, lax.axis_index("tp") * count, count, axis=0)


def sum_rows(partial):
    shares = lax.all_to_all(
        partial.astype(jnp.bfloat16), "tp", split_axis=0, concat_axis=0, tiled=True
    )
    shares = shares.reshape((lax.axis_size("tp"), -1, shares.shape[1]))
    return jnp.sum(shares.astype(jnp.float32), axis=0)


def join_rows(rows):
    return lax.all_gather(rows, "tp", axis=0, tiled=True)


def block_forward(values, gain_vector, weights, width):
    widened, factor, normed = normalize(values, gain_vector)
    pre = project(normed, weights[:, : 2 * width])
    hidden = (jax.nn.silu(pre[:, :width]) * pre[:, width:]).astype(jnp.bfloat16)
    branch = sum_rows(project_back(hidden, weights[:, 2 * width :]))
    return join_rows((own_rows(widened) + 0.5 * branch).astype(jnp.bfloat16))


def block_backward(normalized, cotangent, weights, width):
    widened, factor, normed = normalized
    pre = project(normed, weights[:, : 2 * width])
    gate_pre, up_pre = pre[:, :width], pre[:, width:]
    sigmoid_gate = jax.nn.sigmoid(gate_pre)
    activated = gate_pre * sigmoid_gate
    hidden = (activated * up_pre).astype(jnp.bfloat16)
    hidden_grad = 0.5 * project(cotangent, weights[:, 2 * width :])
    gate_grad = (
        hidden_grad * up_pre * sigmoid_gate * (1.0 + gate_pre * (1.0 - sigmoid_gate))
    ).astype(jnp.bfloat16)
    up_grad = (hidden_grad * activated).astype(jnp.bfloat16)
    pieces = jnp.concatenate((gate_grad, up_grad, hidden), axis=1)
    partial_value = project_back(pieces[:, : 2 * width], weights[:, : 2 * width])
    return (partial_value, pieces)


def backward_rows(normalized, cotangent, gain_vector, partial_value):
    normed_grad = sum_rows(partial_value)
    widened, factor = own_rows(normalized[0]), own_rows(normalized[1])
    scaled = normed_grad * gain_vector
    unit_rows = widened * factor
    rows_grad = own_rows(cotangent).astype(jnp.float32) + factor * (
        scaled - unit_rows * jnp.mean(scaled * unit_rows, axis=-1, keepdims=True)
    )
    return rows_grad.astype(jnp.bfloat16)


def gather_weights(gate, up, down):
    return lax.all_gather(jnp.concatenate((gate, up, down.T), axis=1), "fs", axis=0, tiled=True)


def share_columns(rows):
    return lax.all_to_all(rows, "fs", split_axis=1, concat_axis=0, tiled=True)


def join_columns(share):
    joined = join_rows(share)
    parts = joined.reshape((lax.axis_size("tp"), lax.axis_size("fs"), -1, joined.shape[1]))
    return jnp.swapaxes(parts, 0, 1).reshape(joined.shape)


def per_device_general(
    late_input,
    early_input,
    early_mid,
    cotangent,
    gain_first,
    gain_second,
    gate_first,
    up_first,
    down_first,
    gate_second,
    up_second,
    down_second,
    sum_gate_first,
    sum_up_first,
    sum_down_first,
    sum_gate_second,
    sum_up_second,
    sum_down_second,
):
    width = gate_first.shape[1]
    weights_second = gather_weights(gate_second, up_second, down_second)
    weights_first = gather_weights(gate_first, up_first, down_first)
    norm_second = normalize(early_mid, gain_second)
    norm_first = normalize(early_input, gain_first)
    early_rows = jnp.stack(
        (own_rows(norm_second[2]), own_rows(norm_first[2]), own_rows(cotangent))
    )
    early_shares = lax.all_to_all(early_rows, "fs", split_axis=2, concat_axis=1, tiled=True)
    columns_second = join_columns(early_shares[0])
    columns_first = join_columns(early_shares[1])
    columns_cotangent = join_columns(early_shares[2])
    partial_second, pieces_second = block_backward(
        norm_second, cotangent, weights_second, width
    )
    all_second = lax.all_gather(pieces_second, "fs", axis=0, tiled=True)
    mid_rows = backward_rows(norm_second, cotangent, gain_second, partial_second)
    mid_grad = join_rows(mid_rows)
    columns_mid = join_columns(share_columns(mid_rows))
    partial_first, pieces_first = block_backward(norm_first, mid_grad, weights_first, width)
    all_first = lax.all_gather(pieces_first, "fs", axis=0, tiled=True)
    late_mid = block_forward(late_input, gain_first, weights_first, width)
    input_grad = join_rows(backward_rows(norm_first, mid_grad, gain_first, partial_first))
    late_out = block_forward(late_mid, gain_second, weights_second, width)

    def collect(pieces, columns_in, columns_out, sums):
        return (
            sums[0] + fold_rows(columns_in, pieces[:, :width]),
            sums[1] + fold_rows(columns_in, pieces[:, width : 2 * width]),
            sums[2] + 0.5 * fold_rows(pieces[:, 2 * width :], columns_out),
        )

    new_second = collect(
        all_second, columns_second, columns_cotangent, (sum_gate_second, sum_up_second, sum_down_second)
    )
    new_first = collect(
        all_first, columns_first, columns_mid, (sum_gate_first, sum_up_first, sum_down_first)
    )
    return (late_mid, late_out, input_grad) + new_first + new_second


def solution(mesh):
    rows, up_down, down_up = P("fs", None), P("fs", "tp"), P("tp", "fs")
    weights = (up_down, up_down, down_up)
    in_specs = (rows,) * 4 + (P(), P()) + weights * 4
    out_specs = (rows,) * 3 + weights * 2
    line_of_four = mesh.shape["fs"] == PLANES * CORES and mesh.shape["tp"] == TP
    body = per_device if line_of_four else per_device_general
    return jax.shard_map(
        body, mesh=mesh, in_specs=in_specs, out_specs=out_specs, check_vma=False
    )
```

```python
import functools

import jax
import jax.numpy as jnp
from jax import lax
from jax.experimental import pallas as pl
from jax.experimental.pallas import tpu as pltpu
from jax.sharding import PartitionSpec as P

norm_eps = 1e-06
CORES = 2
TP = 4
PLANES = 4

NT = (((1,), (1,)), ((), ()))
NN = (((1,), (0,)), ((), ()))
TN = (((0,), (0,)), ((), ()))


def mm(left, right, dims):
    return lax.dot_general(left, right, dims, preferred_element_type=jnp.float32)


def norm_parts(rows):
    wide = rows.astype(jnp.float32)
    factor = lax.rsqrt(jnp.mean(wide * wide, axis=-1, keepdims=True) + norm_eps)
    return wide, factor


def step_kernel(
    late_in, mid_in, cot_in, early_in, gain2, gain1,
    gate2, up2, down2, gate1, up1, down1,
    late_mid, late_out, grad_in, grads2, grads1,
    weights, acts, late, normed, late_normed, pieces, pieces_in, cols_in,
    part, part_in2, part_in1, late_part, late_part_in, sent, back_rows, done_rows,
    own_grads, acc, late_acc, late_hid, send_sems, recv_sems, local_sems, ack,
):
    f, t = lax.axis_index("fs"), lax.axis_index("tp")
    z, core = f // CORES, f % CORES
    peer = 1 - core
    inner = (z == 1) | (z == 2)
    outer = (z == 0) | (z == 3)
    near, upper = (z // 2) * 3, z // 2
    q = late_in.shape[0] // TP
    rows = PLANES * q
    half = 2 * q
    hidden, width = down2.shape
    tile = TP * half
    grads = (grads2, grads1)
    shards = ((gate2, up2, down2), (gate1, up1, down1))
    out_rows = (late_mid, late_out, grad_in)
    gains = (gain2, gain1)
    ids = {}

    def sem(name):
        return ids.setdefault(name, len(ids))

    def column(mask):
        x, y = t % 2, t // 2
        gx, gy = mask % 2, mask // 2
        x = x + gx - 2 * x * gx
        y = y + gy - 2 * y * gy
        return y * 2 + x

    def device(zz, cc, tt):
        return (zz * CORES + cc, tt)

    def remote(src, dst, index, where):
        return pltpu.make_async_remote_copy(
            src_ref=src, dst_ref=dst, send_sem=send_sems.at[index],
            recv_sem=recv_sems.at[index], device_id=where,
            device_id_type=pl.DeviceIdType.MESH,
        )

    def local(src, dst, index):
        return pltpu.make_async_copy(src, dst, local_sems.at[index])

    def own_quarter(tt):
        return pl.ds(pl.multiple_of(tt * q, q), q)

    def feature(slot, other):
        v = slot + (1 - slot // 2) * (1 - 2 * slot)
        zs = v + upper * (3 - 2 * v)
        cc = core + other - 2 * core * other
        return pl.ds(pl.multiple_of((zs * CORES + cc) * width, width), width)

    barrier = pltpu.get_barrier_semaphore()
    friends = [device((z + k) % PLANES, core, t) for k in range(1, PLANES)]
    friends += [device(z, peer, t)] + [device(z, core, column(m)) for m in range(1, TP)]
    for friend in friends:
        pl.semaphore_signal(barrier, inc=1, device_id=friend, device_id_type=pl.DeviceIdType.MESH)
    pl.semaphore_wait(barrier, len(friends))

    mine = own_quarter(t)
    parts = [pl.ds(j * hidden, hidden) for j in range(3)]

    def row_item(name, ref, store):
        return (name, ref.at[mine], lambda s: store.at[pl.ds(s * q, q)])

    def shard_item(b, j):
        return (("w", b, j), shards[b][j], lambda s: weights.at[b, s, parts[j]])

    z_items = [row_item("m", mid_in, acts.at[0, 0]), row_item("c", cot_in, acts.at[1, 0])]
    z_items += [shard_item(0, 0), shard_item(0, 1)]
    z_items += [row_item("e", early_in, acts.at[2, 0]), row_item("l", late_in, late.at[0, 0])]
    z_items += [shard_item(0, 2)]
    z_items += [shard_item(1, j) for j in range(3)]
    z_base = {}
    for name, _, _ in z_items:
        z_base[name] = sem((name, 0))
        for s in range(1, 4):
            sem((name, s))

    def z_copy(item, s, where):
        name, src, to = item
        return remote(src, to(s), z_base[name] + s, where)

    first_target = device(1 + upper, core, t)
    second_target = device(2 - upper, core, t)
    mid_target = device(3 - z, core, t)

    def outer_sends():
        out = []
        for item in z_items:
            out.append(z_copy(item, 1, first_target))
            if item[0] != "l":
                out.append(z_copy(item, 3, second_target))
        return out

    def inner_sends():
        return [z_copy(item, 2, mid_target) for item in z_items if item[0] != "l"]

    out_dev = device(near, core, t)

    def grad_back(b, j):
        return remote(sent.at[b, j], grads[b].at[j], sem(("g", b, j)), out_dev)

    def row_source(k):
        return (late.at[1, 0], done_rows.at[0], done_rows.at[1])[k]

    def rows_back(k):
        return remote(row_source(k).at[pl.ds(q, q)], back_rows.at[k], sem(("r", k)), out_dev)

    def deliver(k, m, src):
        return remote(src, out_rows[k].at[mine], sem(("d", k, m)), device(z, core, column(m)))

    def keep_rows(k, src):
        return local(src, out_rows[k].at[mine], 22 + k)

    def deliver_wait(k, m):
        other = column(m)
        dst = out_rows[k].at[own_quarter(other)]
        remote(dst, dst, sem(("d", k, m)), device(z, core, other)).wait_recv()

    for b in range(2):
        for j in range(3):
            sem(("g", b, j))
    for k in range(3):
        sem(("r", k))
        for m in range(1, TP):
            sem(("d", k, m))

    @pl.when(outer)
    def _():
        for copy in outer_sends():
            copy.start()
        for k in (0, 2, 1):
            rows_back(k).wait_recv()
            for m in range(1, TP):
                deliver(k, m, back_rows.at[k]).start()
            keep_rows(k, back_rows.at[k]).start()
        for copy in outer_sends():
            copy.wait_send()
        for k in range(3):
            keep_rows(k, back_rows.at[k]).wait()
        for b in range(2):
            for j in range(3):
                grad_back(b, j).wait_recv()
        for k in range(3):
            for m in range(1, TP):
                deliver(k, m, back_rows.at[k]).wait_send()
                deliver_wait(k, m)

    @pl.when(inner)
    def _():
        for copy in inner_sends():
            copy.start()
        peer_dev = device(z, peer, t)

        def shard_local(b, j):
            return local(shards[b][j], weights.at[b, 0, parts[j]], 3 * b + j)

        w_base = []
        for b in range(2):
            w_base.append([])
            for j in range(3):
                w_base[b].append(sem(("p", b, j, 0)))
                for s in range(1, 4):
                    sem(("p", b, j, s))

        def shard_forward(b, j, s, src):
            return remote(src, weights.at[b, 4 + s, parts[j]], w_base[b][j] + s, peer_dev)

        def row_locals(a):
            src = (mid_in, cot_in, early_in, late_in)[a]
            out = []
            for m in range(TP):
                dst = late.at[0, m, pl.ds(0, q)] if a == 3 else acts.at[a, m, pl.ds(0, q)]
                out.append(local(src.at[own_quarter(column(m))], dst, 6 + TP * a + m))
            return out

        for a in range(4):
            for copy in row_locals(a):
                copy.start()
        for b in range(2):
            for j in range(3):
                shard_local(b, j).start()
                shard_forward(b, j, 0, shards[b][j]).start()

        def spread_rows(a):
            src = (acts.at[a, 0], late.at[0, 0])[a == 3].at[pl.ds(q, q if a == 3 else 3 * q)]
            out = []
            for m in range(1, TP):
                full = late.at[0, m] if a == 3 else acts.at[a, m]
                dst = full.at[pl.ds(q, q if a == 3 else 3 * q)]
                out.append(remote(src, dst, sem(("s", a, m)), device(z, core, column(m))))
            return out

        def z_arrived(index, s):
            item = z_items[index]
            remote(item[2](s), item[2](s), z_base[item[0]] + s, mid_target).wait_recv()

        def gather_rows(a, index):
            for s in (1,) if a == 3 else (1, 2, 3):
                z_arrived(index, s)
            for copy in spread_rows(a):
                copy.start()

        def rows_ready(a):
            for copy in row_locals(a):
                copy.wait()
            for copy in spread_rows(a):
                copy.wait_recv()

        gather_rows(0, 0)
        gather_rows(1, 1)

        def normalize_block(b):
            @pl.loop(0, TP * PLANES)
            def _(i):
                at = pl.ds(pl.multiple_of((i % PLANES) * q, q), q)
                wide, factor = norm_parts(acts[2 * b, i // PLANES, at, :])
                normed[i // PLANES, at, :] = (wide * factor * gains[b][...]).astype(jnp.bfloat16)

        def rows_of(ref, h, cols):
            at = pl.ds(pl.multiple_of(h * half, half), half)
            return ref[:, at, cols].reshape(tile, width)

        def take_part(b, j, slot, other):
            @pl.when((slot == 0) & (other == 0))
            def _():
                shard_local(b, j).wait()

            @pl.when((slot > 0) & (other == 0))
            def _():
                ref = weights.at[b, slot, parts[j]]
                remote(ref, ref, z_base[("w", b, j)] + slot, mid_target).wait_recv()
                shard_forward(b, j, slot, ref).start()

            @pl.when(other == 1)
            def _():
                ref = weights.at[b, 4 + slot, parts[j]]
                remote(ref, ref, w_base[b][j] + slot, peer_dev).wait_recv()

        def pre_block(b, first, end):
            if first == 0:
                acc[...] = jnp.zeros_like(acc)

            @pl.loop(first, end)
            def _(i):
                slot, other = i // 2, i % 2
                for j in range(2):
                    take_part(b, j, slot, other)
                at = slot + 4 * other
                cols = feature(slot, other)

                @pl.loop(0, 2)
                def _(h):
                    piece = rows_of(normed, h, cols)
                    for j in range(2):
                        acc[j, h] += mm(piece, weights[b, at, parts[j], :], NT)

        def down_shard(b, slot, other):
            cots = acts.at[2 * b + 1]
            cols = feature(slot, other)

            @pl.loop(0, 2)
            def _(h):
                w = weights[b, slot + 4 * other, parts[2], :]
                late_acc[h] += mm(rows_of(cots, h, cols), w, NT)

        def down_block(b):
            late_acc[...] = jnp.zeros_like(late_acc)

            @pl.loop(0, 8)
            def _(i):
                take_part(b, 2, i // 2, i % 2)
                down_shard(b, i // 2, i % 2)

        def pieces_block(h):
            @pl.loop(0, TP)
            def _(m):
                at = pl.ds(pl.multiple_of(m * half, half), half)
                to = pl.ds(pl.multiple_of(h * half, half), half)
                gate, up = acc[0, h, at, :], acc[1, h, at, :]
                grad = 0.5 * late_acc[h, at, :]
                sig = 1.0 / (1.0 + jnp.exp(-gate))
                act = gate * sig
                turn = sig * (1.0 + gate * (1.0 - sig))
                pieces[0, m, to, :] = (grad * up * turn).astype(jnp.bfloat16)
                pieces[1, m, to, :] = (grad * act).astype(jnp.bfloat16)
                pieces[2, m, to, :] = (act * up).astype(jnp.bfloat16)

        def swaps(b):
            out = []
            for j in range(3):
                out.append(remote(pieces.at[j], pieces_in.at[j], sem(("x", b, j)), peer_dev))
            for k in range(2):
                cols = feature(k, 1)
                for j, src in enumerate((normed, acts.at[2 * b + 1])):
                    out.append(
                        remote(src.at[:, :, cols], cols_in.at[j, k], sem(("y", b, j, k)), peer_dev)
                    )
            return out

        def part_copy(r, m):
            at = pl.ds(r * q, q)
            return remote(
                part.at[m, at], part_in1.at[m - 1, at], sem(("n", r, m)),
                device(z, core, column(m)),
            )

        lanes = (pl.ds(0, normed.shape[2] // 2), pl.ds(normed.shape[2] // 2, normed.shape[2] // 2))

        def part_first(h, columns=(1, 2), kinds=(0, 1)):
            at = pl.ds(h * half, half)
            out = []
            for m in columns:
                for kind in kinds:
                    block, slot = ((m, m - 1), (3, 2))[kind]
                    out.append(
                        remote(
                            part.at[block, at, lanes[m - 1]], part_in2.at[slot, at, lanes[m - 1]],
                            sem(("o", h, m, slot)), device(z, core, column(m)),
                        )
                    )
            return out

        def part_second(h, columns=(1, 2)):
            at = pl.ds(h * half, half)
            return [
                remote(
                    part.at[3 - m, at, lanes[m - 1]], part_in2.at[2 - m, at, lanes[m - 1]],
                    sem(("t", h, m)), device(z, core, column(3 - m)),
                )
                for m in columns
            ]

        def part_merge(h):
            at = pl.ds(h * half, half)
            for m in (1, 2):
                part_first(h, (m,), (1,))[0].wait_recv()
                mine_too = part[3 - m, at, lanes[m - 1]].astype(jnp.float32)
                other = part_in2[2, at, lanes[m - 1]].astype(jnp.float32)
                part[3 - m, at, lanes[m - 1]] = (mine_too + other).astype(jnp.bfloat16)
                part_second(h, (m,))[0].start()

        def grad_part(b, h):
            at = pl.ds(h * half, half)

            @pl.loop(0, 8)
            def _(i):
                cols = feature(i % 4, i // 4)
                total = None
                for j in range(2):
                    left = pieces[j, :, at, :].reshape(tile, hidden)
                    one = mm(left, weights[b, i, parts[j], :], NN)
                    total = one if j == 0 else total + one
                part[:, at, cols] = total.astype(jnp.bfloat16).reshape(TP, half, width)

        def fold(b):
            for copy in swaps(b):
                copy.wait_recv()
            tokens = TP * rows
            cots = acts.at[2 * b + 1]
            for k in (1, 0):
                cols = feature(k, 0)
                out = (own_grads, sent)[k].at[b]
                sides = (
                    (normed[:, :, cols].reshape(tokens, width), cols_in[0, k].reshape(tokens, width)),
                    (cots[:, :, cols].reshape(tokens, width), cols_in[1, k].reshape(tokens, width)),
                )
                for j in range(3):
                    own, other = sides[j // 2]
                    one = mm(pieces[j].reshape(tokens, hidden), own, TN)
                    one = one + mm(pieces_in[j].reshape(tokens, hidden), other, TN)
                    out[j] = (one if j < 2 else 0.5 * one).astype(jnp.bfloat16)
                    if k == 1 and (b == 0 or j < 2):
                        grad_back(b, j).start()
            keep_grads(b).start()

        def keep_grads(b):
            return local(own_grads.at[b], grads[b], 25 + b)

        def keep_late(m):
            at = own_quarter(column(m))
            return local(late.at[1, m, pl.ds(0, q)], late_mid.at[at], 27 + m)

        def rows_grad(b, r, out):
            if b == 0:
                copies = part_first(r, kinds=(0,)) + part_second(r)
            else:
                copies = [part_copy(r, m) for m in range(1, TP)]
            for copy in copies:
                copy.wait_recv()
            arrived = (part_in2, part_in1)[b]
            size = half if b == 0 else q
            at = pl.ds(r * size, size)
            total = part[0, at, :].astype(jnp.float32)
            for m in range(1, 3 if b == 0 else TP):
                total = total + arrived[m - 1, at, :].astype(jnp.float32)
            wide, factor = norm_parts(acts[2 * b, 0, at, :])
            scaled = total * gains[b][...]
            unit = wide * factor
            inner_mean = jnp.mean(scaled * unit, axis=-1, keepdims=True)
            cot = acts[2 * b + 1, 0, at, :].astype(jnp.float32)
            out[at, :] = (cot + factor * (scaled - unit * inner_mean)).astype(jnp.bfloat16)

        def mid_copy(h, m):
            at = pl.ds(h * half, half)
            return remote(
                acts.at[3, 0, at], acts.at[3, m, at], sem(("a", h, m)),
                device(z, core, column(m)),
            )

        def mid_forward(h, m):
            at = pl.ds(h * half + (m - 1) * q, q)
            return remote(
                acts.at[3, m, at], acts.at[3, 3, at], sem(("f", h, m)),
                device(z, core, column(3 - m)),
            )

        def mid_pass(h):
            for m in (1, 2):
                mid_copy(h, m).wait_recv()
                mid_forward(h, m).start()

        def late_block(b, n):
            @pl.loop(0, TP * 2)
            def _(i):
                at = pl.ds(pl.multiple_of((i % 2) * q, q), q)
                wide, factor = norm_parts(late[n, i // 2, at, :])
                late_normed[i // 2, at, :] = (wide * factor * gains[b][...]).astype(jnp.bfloat16)

            late_acc[...] = jnp.zeros_like(late_acc)

            @pl.loop(0, 8)
            def _(i):
                cols = feature(i % 4, i // 4)
                piece = late_normed[:, :, cols].reshape(tile, width)
                for j in range(2):
                    late_acc[j] += mm(piece, weights[b, i, parts[j], :], NT)

            gate = late_acc[0]
            hid = (gate / (1.0 + jnp.exp(-gate)) * late_acc[1]).astype(jnp.bfloat16)
            late_hid[...] = hid
            if n == 0:
                late_acc[...] = jnp.zeros_like(late_acc)
                for h in range(2):
                    for m in (1, 2):
                        mid_forward(h, m).wait_recv()

            @pl.loop(0, 8)
            def _(i):
                slot, other = i // 2, i % 2
                if n == 0:
                    take_part(b, 2, slot, other)
                cols = feature(slot, other)
                w = weights[b, slot + 4 * other, parts[2], :]
                one = mm(late_hid[...], w, NN).astype(jnp.bfloat16)
                late_part[:, :, cols] = one.reshape(TP, half, width)
                if n == 0:
                    for m in range(1, TP):
                        late_block_copy(i, m).start()
                    down_shard(b, slot, other)

            if n == 1:
                for r in (1, 0):
                    for m in range(1, TP):
                        late_copy(r, m).start()

        late_base = sem(("b", 0))
        for i in range(1, 24):
            sem(("b", i))

        def late_block_copy(i, m):
            cols = feature(i // 2, i % 2)
            return remote(
                late_part.at[m, :, cols], late_part_in.at[0, m - 1, :, cols],
                late_base + i * 3 + (m - 1), device(z, core, column(m)),
            )

        def late_copy(r, m):
            at = pl.ds(r * q, q)
            return remote(
                late_part.at[m, at], late_part_in.at[1, m - 1, at], sem(("h", r, m)),
                device(z, core, column(m)),
            )

        def late_sum(n, r, out):
            if n == 1:
                for m in range(1, TP):
                    late_copy(r, m).wait_recv()
            at = pl.ds(r * q, q)
            total = late_part[0, at, :].astype(jnp.float32)
            for m in range(1, TP):
                total = total + late_part_in[n, m - 1, at, :].astype(jnp.float32)
            value = late[n, 0, at, :].astype(jnp.float32) + 0.5 * total
            out[at, :] = value.astype(jnp.bfloat16)

        def late_spread(m):
            return remote(
                late.at[1, 0], late.at[1, m], sem(("k", m)), device(z, core, column(m))
            )

        def late_forward(m):
            at = pl.ds((m - 1) * q, q)
            return remote(
                late.at[1, m, at], late.at[1, 3, at], sem(("j", m)), device(z, core, column(3 - m))
            )

        rows_ready(0)
        normalize_block(0)
        pre_block(0, 0, 8)
        rows_ready(1)
        gather_rows(2, 4)
        gather_rows(3, 5)
        down_block(0)
        for h in range(2):
            pieces_block(h)
            grad_part(0, h)
            for copy in part_first(h):
                copy.start()
        for copy in swaps(0):
            copy.start()
        part_merge(0)
        fold(0)
        part_merge(1)
        for copy in swaps(0):
            copy.wait_send()
        pl.semaphore_signal(ack, inc=1, device_id=peer_dev, device_id_type=pl.DeviceIdType.MESH)

        rows_ready(2)
        normalize_block(1)
        for h in range(2):
            rows_grad(0, h, acts.at[3, 0])
            for m in (1, 2):
                mid_copy(h, m).start()
            pre_block(1, 2 * h, 2 + 3 * h)
        mid_pass(0)
        mid_pass(1)
        pre_block(1, 5, 8)
        rows_ready(3)
        late_block(1, 0)

        @pl.loop(0, 2)
        def _(h):
            pieces_block(h)

        pl.semaphore_wait(ack, 1)
        for copy in swaps(1):
            copy.start()

        @pl.loop(0, 8)
        def _(i):
            for m in range(1, TP):
                late_block_copy(i, m).wait_recv()

        late_rows = late.at[1, 0]
        late_sum(0, 1, late_rows)
        late_sum(0, 0, late_rows)
        for m in (1, 2):
            late_spread(m).start()
        rows_back(0).start()
        for h in range(2):
            for copy in part_first(h) + part_second(h):
                copy.wait_send()
        grad_part(1, 0)
        for m in (1, 2):
            late_spread(m).wait_recv()
            late_forward(m).start()
        for r in (1, 0):
            for m in range(1, TP):
                part_copy(r, m).start()
        fold(1)

        @pl.loop(0, 8)
        def _(i):
            for m in range(1, TP):
                late_block_copy(i, m).wait_send()

        for m in (1, 2):
            late_forward(m).wait_recv()
        late_block(0, 1)
        for m in range(TP):
            keep_late(m).start()

        def finish(k):
            src = row_source(k).at[pl.ds(0, q)]
            for m in range(1, TP):
                deliver(k, m, src).start()
            keep_rows(k, src).start()

        rows_grad(1, 1, done_rows.at[1])
        rows_back(2).start()
        rows_grad(1, 0, done_rows.at[1])
        late_sum(1, 1, done_rows.at[0])
        rows_back(1).start()
        grad_back(1, 2).start()
        finish(2)
        late_sum(1, 0, done_rows.at[0])
        finish(1)

        for copy in inner_sends():
            copy.wait_send()
        for b in range(2):
            for j in range(3):
                for s in range(4):
                    src = shards[b][j] if s == 0 else weights.at[b, s, parts[j]]
                    shard_forward(b, j, s, src).wait_send()
                grad_back(b, j).wait_send()
        for a in range(4):
            for copy in spread_rows(a):
                copy.wait_send()
        for copy in swaps(1):
            copy.wait_send()
        for m in range(1, TP):
            for r in range(2):
                part_copy(r, m).wait_send()
                late_copy(r, m).wait_send()
        for m in (1, 2):
            late_spread(m).wait_send()
            late_forward(m).wait_send()
            for h in range(2):
                mid_copy(h, m).wait_send()
                mid_forward(h, m).wait_send()
        for b in range(2):
            keep_grads(b).wait()
        for m in range(TP):
            keep_late(m).wait()
        for k in range(3):
            rows_back(k).wait_send()
            if k > 0:
                keep_rows(k, row_source(k).at[pl.ds(0, q)]).wait()
                for m in range(1, TP):
                    deliver(k, m, row_source(k).at[pl.ds(0, q)]).wait_send()
                    deliver_wait(k, m)


def add_kernel(r0, r1, r2, grads2, grads1, *refs):
    olds, outs = refs[:6], refs[6:]
    for src, dst in zip((r0, r1, r2), outs[:3]):
        dst[...] = src[...]
    for j in range(6):
        grads = (grads1, grads2)[j // 3]
        outs[3 + j][...] = olds[j][...] + grads[j % 3].astype(jnp.float32)


def per_device(
    late_input,
    early_input,
    early_mid,
    cotangent,
    gain_first,
    gain_second,
    gate_first,
    up_first,
    down_first,
    gate_second,
    up_second,
    down_second,
    *sums,
):
    count, feats = late_input.shape
    width, hidden = gate_first.shape
    q = count // TP
    half = 2 * q
    tile = TP * half
    bf = jnp.bfloat16
    anywhere = pl.BlockSpec(memory_space=pl.ANY)
    in_vmem = pl.BlockSpec(memory_space=pltpu.VMEM)
    rows_shape = jax.ShapeDtypeStruct((count, feats), bf)
    grads_shape = jax.ShapeDtypeStruct((3, hidden, width), bf)
    outs = pl.pallas_call(
        step_kernel,
        out_shape=[rows_shape] * 3 + [grads_shape] * 2,
        in_specs=[anywhere] * 4 + [in_vmem] * 2 + [anywhere] * 6,
        out_specs=[anywhere] * 5,
        scratch_shapes=[
            pltpu.VMEM((2, 8, 3 * hidden, width), bf),
            pltpu.VMEM((4, TP, count, feats), bf),
            pltpu.VMEM((2, TP, half, feats), bf),
            pltpu.VMEM((TP, count, feats), bf),
            pltpu.VMEM((TP, half, feats), bf),
            pltpu.VMEM((3, TP, count, hidden), bf),
            pltpu.VMEM((3, TP, count, hidden), bf),
            pltpu.VMEM((2, 2, TP, count, width), bf),
            pltpu.VMEM((TP, count, feats), bf),
            pltpu.VMEM((3, count, feats), bf),
            pltpu.VMEM((3, half, feats), bf),
            pltpu.VMEM((TP, half, feats), bf),
            pltpu.VMEM((2, 3, half, feats), bf),
            pltpu.VMEM((2, 3, hidden, width), bf),
            pltpu.VMEM((3, q, feats), bf),
            pltpu.VMEM((2, half, feats), bf),
            pltpu.VMEM((2, 3, hidden, width), bf),
            pltpu.VMEM((2, 2, tile, hidden), jnp.float32),
            pltpu.VMEM((2, tile, hidden), jnp.float32),
            pltpu.VMEM((tile, hidden), bf),
            pltpu.SemaphoreType.DMA((208,)),
            pltpu.SemaphoreType.DMA((208,)),
            pltpu.SemaphoreType.DMA((31,)),
            pltpu.SemaphoreType.REGULAR,
        ],
        compiler_params=pltpu.CompilerParams(
            collective_id=0, has_side_effects=True, vmem_limit_bytes=67043328
        ),
        name="step",
    )(
        late_input, early_mid, cotangent, early_input,
        gain_second.reshape((1, -1)), gain_first.reshape((1, -1)),
        gate_second.T, up_second.T, down_second,
        gate_first.T, up_first.T, down_first,
    )
    tall = [old.T if j % 3 < 2 else old for j, old in enumerate(sums)]
    steps = 4
    row_spec = pl.BlockSpec((count // steps, feats), lambda i: (i, 0))
    sum_spec = pl.BlockSpec((hidden // steps, width), lambda i: (i, 0))
    grad_spec = pl.BlockSpec((3, hidden // steps, width), lambda i: (0, i, 0))
    done = pl.pallas_call(
        add_kernel,
        grid=(steps,),
        out_shape=[rows_shape] * 3 + [jax.ShapeDtypeStruct((hidden, width), jnp.float32)] * 6,
        in_specs=[row_spec] * 3 + [grad_spec] * 2 + [sum_spec] * 6,
        out_specs=[row_spec] * 3 + [sum_spec] * 6,
        name="add",
    )(*outs, *tall)
    fresh = [new.T if j % 3 < 2 else new for j, new in enumerate(done[3:])]
    return tuple(done[:3]) + tuple(fresh)


def normalize(values, gain_vector):
    widened = values.astype(jnp.float32)
    factor = lax.rsqrt(jnp.mean(widened * widened, axis=-1, keepdims=True) + norm_eps)
    normed = (widened * factor * gain_vector).astype(jnp.bfloat16)
    return (widened, factor, normed)


def project(rows, weights):
    return jnp.dot(rows, weights, preferred_element_type=jnp.float32)


def project_back(hidden_rows, weights):
    return jnp.einsum("tf,df->td", hidden_rows, weights, preferred_element_type=jnp.float32)


def fold_rows(left, right):
    return jnp.einsum("ta,tb->ab", left, right, preferred_element_type=jnp.float32)


def own_rows(rows):
    count = rows.shape[0] // lax.axis_size("tp")
    return lax.dynamic_slice_in_dim(rows, lax.axis_index("tp") * count, count, axis=0)


def sum_rows(partial):
    shares = lax.all_to_all(
        partial.astype(jnp.bfloat16), "tp", split_axis=0, concat_axis=0, tiled=True
    )
    shares = shares.reshape((lax.axis_size("tp"), -1, shares.shape[1]))
    return jnp.sum(shares.astype(jnp.float32), axis=0)


def join_rows(rows):
    return lax.all_gather(rows, "tp", axis=0, tiled=True)


def block_forward(values, gain_vector, weights, width):
    widened, factor, normed = normalize(values, gain_vector)
    pre = project(normed, weights[:, : 2 * width])
    hidden = (jax.nn.silu(pre[:, :width]) * pre[:, width:]).astype(jnp.bfloat16)
    branch = sum_rows(project_back(hidden, weights[:, 2 * width :]))
    return join_rows((own_rows(widened) + 0.5 * branch).astype(jnp.bfloat16))


def block_backward(normalized, cotangent, weights, width):
    widened, factor, normed = normalized
    pre = project(normed, weights[:, : 2 * width])
    gate_pre, up_pre = pre[:, :width], pre[:, width:]
    sigmoid_gate = jax.nn.sigmoid(gate_pre)
    activated = gate_pre * sigmoid_gate
    hidden = (activated * up_pre).astype(jnp.bfloat16)
    hidden_grad = 0.5 * project(cotangent, weights[:, 2 * width :])
    gate_grad = (
        hidden_grad * up_pre * sigmoid_gate * (1.0 + gate_pre * (1.0 - sigmoid_gate))
    ).astype(jnp.bfloat16)
    up_grad = (hidden_grad * activated).astype(jnp.bfloat16)
    pieces = jnp.concatenate((gate_grad, up_grad, hidden), axis=1)
    partial_value = project_back(pieces[:, : 2 * width], weights[:, : 2 * width])
    return (partial_value, pieces)


def backward_rows(normalized, cotangent, gain_vector, partial_value):
    normed_grad = sum_rows(partial_value)
    widened, factor = own_rows(normalized[0]), own_rows(normalized[1])
    scaled = normed_grad * gain_vector
    unit_rows = widened * factor
    rows_grad = own_rows(cotangent).astype(jnp.float32) + factor * (
        scaled - unit_rows * jnp.mean(scaled * unit_rows, axis=-1, keepdims=True)
    )
    return rows_grad.astype(jnp.bfloat16)


def gather_weights(gate, up, down):
    return lax.all_gather(jnp.concatenate((gate, up, down.T), axis=1), "fs", axis=0, tiled=True)


def share_columns(rows):
    return lax.all_to_all(rows, "fs", split_axis=1, concat_axis=0, tiled=True)


def join_columns(share):
    joined = join_rows(share)
    parts = joined.reshape((lax.axis_size("tp"), lax.axis_size("fs"), -1, joined.shape[1]))
    return jnp.swapaxes(parts, 0, 1).reshape(joined.shape)


def per_device_general(
    late_input,
    early_input,
    early_mid,
    cotangent,
    gain_first,
    gain_second,
    gate_first,
    up_first,
    down_first,
    gate_second,
    up_second,
    down_second,
    sum_gate_first,
    sum_up_first,
    sum_down_first,
    sum_gate_second,
    sum_up_second,
    sum_down_second,
):
    width = gate_first.shape[1]
    weights_second = gather_weights(gate_second, up_second, down_second)
    weights_first = gather_weights(gate_first, up_first, down_first)
    norm_second = normalize(early_mid, gain_second)
    norm_first = normalize(early_input, gain_first)
    early_rows = jnp.stack(
        (own_rows(norm_second[2]), own_rows(norm_first[2]), own_rows(cotangent))
    )
    early_shares = lax.all_to_all(early_rows, "fs", split_axis=2, concat_axis=1, tiled=True)
    columns_second = join_columns(early_shares[0])
    columns_first = join_columns(early_shares[1])
    columns_cotangent = join_columns(early_shares[2])
    partial_second, pieces_second = block_backward(
        norm_second, cotangent, weights_second, width
    )
    all_second = lax.all_gather(pieces_second, "fs", axis=0, tiled=True)
    mid_rows = backward_rows(norm_second, cotangent, gain_second, partial_second)
    mid_grad = join_rows(mid_rows)
    columns_mid = join_columns(share_columns(mid_rows))
    partial_first, pieces_first = block_backward(norm_first, mid_grad, weights_first, width)
    all_first = lax.all_gather(pieces_first, "fs", axis=0, tiled=True)
    late_mid = block_forward(late_input, gain_first, weights_first, width)
    input_grad = join_rows(backward_rows(norm_first, mid_grad, gain_first, partial_first))
    late_out = block_forward(late_mid, gain_second, weights_second, width)

    def collect(pieces, columns_in, columns_out, sums):
        return (
            sums[0] + fold_rows(columns_in, pieces[:, :width]),
            sums[1] + fold_rows(columns_in, pieces[:, width : 2 * width]),
            sums[2] + 0.5 * fold_rows(pieces[:, 2 * width :], columns_out),
        )

    new_second = collect(
        all_second, columns_second, columns_cotangent, (sum_gate_second, sum_up_second, sum_down_second)
    )
    new_first = collect(
        all_first, columns_first, columns_mid, (sum_gate_first, sum_up_first, sum_down_first)
    )
    return (late_mid, late_out, input_grad) + new_first + new_second


def solution(mesh):
    rows, up_down, down_up = P("fs", None), P("fs", "tp"), P("tp", "fs")
    weights = (up_down, up_down, down_up)
    in_specs = (rows,) * 4 + (P(), P()) + weights * 4
    out_specs = (rows,) * 3 + weights * 2
    line_of_four = mesh.shape["fs"] == PLANES * CORES and mesh.shape["tp"] == TP
    body = per_device if line_of_four else per_device_general
    return jax.shard_map(
        body, mesh=mesh, in_specs=in_specs, out_specs=out_specs, check_vma=False
    )
```

```python
import functools

import jax
import jax.numpy as jnp
from jax import lax
from jax.experimental import pallas as pl
from jax.experimental.pallas import tpu as pltpu
from jax.sharding import PartitionSpec as P

norm_eps = 1e-06
CORES = 2
TP = 4
PLANES = 4

NT = (((1,), (1,)), ((), ()))
NN = (((1,), (0,)), ((), ()))
TN = (((0,), (0,)), ((), ()))


def mm(left, right, dims):
    return lax.dot_general(left, right, dims, preferred_element_type=jnp.float32)


def norm_parts(rows):
    wide = rows.astype(jnp.float32)
    factor = lax.rsqrt(jnp.mean(wide * wide, axis=-1, keepdims=True) + norm_eps)
    return wide, factor


def step_kernel(
    late_in, mid_in, cot_in, early_in, gain2, gain1,
    gate2, up2, down2, gate1, up1, down1,
    late_mid, late_out, grad_in, grads2, grads1,
    weights, acts, late, normed, late_normed, pieces, pieces_in, cols_in,
    part, part_in2, part_in1, late_part, late_part_in, sent, back_rows, done_rows,
    own_grads, acc, late_acc, late_hid, send_sems, recv_sems, local_sems, ack,
):
    f, t = lax.axis_index("fs"), lax.axis_index("tp")
    z, core = f // CORES, f % CORES
    peer = 1 - core
    inner = (z == 1) | (z == 2)
    outer = (z == 0) | (z == 3)
    near, upper = (z // 2) * 3, z // 2
    q = late_in.shape[0] // TP
    rows = PLANES * q
    half = 2 * q
    hidden, width = down2.shape
    tile = TP * half
    grads = (grads2, grads1)
    shards = ((gate2, up2, down2), (gate1, up1, down1))
    out_rows = (late_mid, late_out, grad_in)
    gains = (gain2, gain1)
    ids = {}

    def sem(name):
        return ids.setdefault(name, len(ids))

    def column(mask):
        x, y = t % 2, t // 2
        gx, gy = mask % 2, mask // 2
        x = x + gx - 2 * x * gx
        y = y + gy - 2 * y * gy
        return y * 2 + x

    def device(zz, cc, tt):
        return (zz * CORES + cc, tt)

    def remote(src, dst, index, where):
        return pltpu.make_async_remote_copy(
            src_ref=src, dst_ref=dst, send_sem=send_sems.at[index],
            recv_sem=recv_sems.at[index], device_id=where,
            device_id_type=pl.DeviceIdType.MESH,
        )

    def local(src, dst, index):
        return pltpu.make_async_copy(src, dst, local_sems.at[index])

    def own_quarter(tt):
        return pl.ds(pl.multiple_of(tt * q, q), q)

    def feature(slot, other):
        v = slot + (1 - slot // 2) * (1 - 2 * slot)
        zs = v + upper * (3 - 2 * v)
        cc = core + other - 2 * core * other
        return pl.ds(pl.multiple_of((zs * CORES + cc) * width, width), width)

    barrier = pltpu.get_barrier_semaphore()
    friends = [device((z + k) % PLANES, core, t) for k in range(1, PLANES)]
    friends += [device(z, peer, t)] + [device(z, core, column(m)) for m in range(1, TP)]
    for friend in friends:
        pl.semaphore_signal(barrier, inc=1, device_id=friend, device_id_type=pl.DeviceIdType.MESH)
    pl.semaphore_wait(barrier, len(friends))

    mine = own_quarter(t)
    parts = [pl.ds(j * hidden, hidden) for j in range(3)]

    def row_item(name, ref, store):
        return (name, ref.at[mine], lambda s: store.at[pl.ds(s * q, q)])

    def shard_item(b, j):
        return (("w", b, j), shards[b][j], lambda s: weights.at[b, s, parts[j]])

    z_items = [row_item("m", mid_in, acts.at[0, 0]), row_item("c", cot_in, acts.at[1, 0])]
    z_items += [shard_item(0, 0), shard_item(0, 1)]
    z_items += [row_item("e", early_in, acts.at[2, 0]), row_item("l", late_in, late.at[0, 0])]
    z_items += [shard_item(0, 2)]
    z_items += [shard_item(1, j) for j in range(3)]
    z_base = {}
    for name, _, _ in z_items:
        z_base[name] = sem((name, 0))
        for s in range(1, 4):
            sem((name, s))

    def z_copy(item, s, where):
        name, src, to = item
        return remote(src, to(s), z_base[name] + s, where)

    first_target = device(1 + upper, core, t)
    second_target = device(2 - upper, core, t)
    mid_target = device(3 - z, core, t)

    def outer_sends():
        out = []
        for item in z_items:
            out.append(z_copy(item, 1, first_target))
            if item[0] != "l":
                out.append(z_copy(item, 3, second_target))
        return out

    def inner_sends():
        return [z_copy(item, 2, mid_target) for item in z_items if item[0] != "l"]

    out_dev = device(near, core, t)

    def grad_back(b, j):
        return remote(sent.at[b, j], grads[b].at[j], sem(("g", b, j)), out_dev)

    def row_source(k):
        return (late.at[1, 0], done_rows.at[0], done_rows.at[1])[k]

    def rows_back(k):
        return remote(row_source(k).at[pl.ds(q, q)], back_rows.at[k], sem(("r", k)), out_dev)

    def deliver(k, m, src):
        return remote(src, out_rows[k].at[mine], sem(("d", k, m)), device(z, core, column(m)))

    def keep_rows(k, src):
        return local(src, out_rows[k].at[mine], 22 + k)

    def deliver_wait(k, m):
        other = column(m)
        dst = out_rows[k].at[own_quarter(other)]
        remote(dst, dst, sem(("d", k, m)), device(z, core, other)).wait_recv()

    for b in range(2):
        for j in range(3):
            sem(("g", b, j))
    for k in range(3):
        sem(("r", k))
        for m in range(1, TP):
            sem(("d", k, m))

    @pl.when(outer)
    def _():
        for copy in outer_sends():
            copy.start()
        for k in (0, 2, 1):
            rows_back(k).wait_recv()
            for m in range(1, TP):
                deliver(k, m, back_rows.at[k]).start()
            keep_rows(k, back_rows.at[k]).start()
        for copy in outer_sends():
            copy.wait_send()
        for k in range(3):
            keep_rows(k, back_rows.at[k]).wait()
        for b in range(2):
            for j in range(3):
                grad_back(b, j).wait_recv()
        for k in range(3):
            for m in range(1, TP):
                deliver(k, m, back_rows.at[k]).wait_send()
                deliver_wait(k, m)

    @pl.when(inner)
    def _():
        for copy in inner_sends():
            copy.start()
        peer_dev = device(z, peer, t)

        def shard_local(b, j):
            return local(shards[b][j], weights.at[b, 0, parts[j]], 3 * b + j)

        w_base = []
        for b in range(2):
            w_base.append([])
            for j in range(3):
                w_base[b].append(sem(("p", b, j, 0)))
                for s in range(1, 4):
                    sem(("p", b, j, s))

        def shard_forward(b, j, s, src):
            return remote(src, weights.at[b, 4 + s, parts[j]], w_base[b][j] + s, peer_dev)

        def row_locals(a):
            src = (mid_in, cot_in, early_in, late_in)[a]
            out = []
            for m in range(TP):
                dst = late.at[0, m, pl.ds(0, q)] if a == 3 else acts.at[a, m, pl.ds(0, q)]
                out.append(local(src.at[own_quarter(column(m))], dst, 6 + TP * a + m))
            return out

        for a in range(4):
            for copy in row_locals(a):
                copy.start()
        for b in range(2):
            for j in range(3):
                shard_local(b, j).start()
                shard_forward(b, j, 0, shards[b][j]).start()

        def spread_rows(a):
            src = (acts.at[a, 0], late.at[0, 0])[a == 3].at[pl.ds(q, q if a == 3 else 3 * q)]
            out = []
            for m in range(1, TP):
                full = late.at[0, m] if a == 3 else acts.at[a, m]
                dst = full.at[pl.ds(q, q if a == 3 else 3 * q)]
                out.append(remote(src, dst, sem(("s", a, m)), device(z, core, column(m))))
            return out

        def z_arrived(index, s):
            item = z_items[index]
            remote(item[2](s), item[2](s), z_base[item[0]] + s, mid_target).wait_recv()

        def gather_rows(a, index):
            for s in (1,) if a == 3 else (1, 2, 3):
                z_arrived(index, s)
            for copy in spread_rows(a):
                copy.start()

        def rows_ready(a):
            for copy in row_locals(a):
                copy.wait()
            for copy in spread_rows(a):
                copy.wait_recv()

        gather_rows(0, 0)
        gather_rows(1, 1)

        def normalize_block(b):
            @pl.loop(0, TP * PLANES)
            def _(i):
                at = pl.ds(pl.multiple_of((i % PLANES) * q, q), q)
                wide, factor = norm_parts(acts[2 * b, i // PLANES, at, :])
                normed[i // PLANES, at, :] = (wide * factor * gains[b][...]).astype(jnp.bfloat16)

        def rows_of(ref, h, cols):
            at = pl.ds(pl.multiple_of(h * half, half), half)
            return ref[:, at, cols].reshape(tile, width)

        def take_part(b, j, slot, other):
            @pl.when((slot == 0) & (other == 0))
            def _():
                shard_local(b, j).wait()

            @pl.when((slot > 0) & (other == 0))
            def _():
                ref = weights.at[b, slot, parts[j]]
                remote(ref, ref, z_base[("w", b, j)] + slot, mid_target).wait_recv()
                shard_forward(b, j, slot, ref).start()

            @pl.when(other == 1)
            def _():
                ref = weights.at[b, 4 + slot, parts[j]]
                remote(ref, ref, w_base[b][j] + slot, peer_dev).wait_recv()

        def pre_block(b, first, end):
            if first == 0:
                acc[...] = jnp.zeros_like(acc)

            @pl.loop(first, end)
            def _(i):
                slot, other = i // 2, i % 2
                for j in range(2):
                    take_part(b, j, slot, other)
                at = slot + 4 * other
                cols = feature(slot, other)

                @pl.loop(0, 2)
                def _(h):
                    piece = rows_of(normed, h, cols)
                    for j in range(2):
                        acc[j, h] += mm(piece, weights[b, at, parts[j], :], NT)

        def down_shard(b, slot, other):
            cots = acts.at[2 * b + 1]
            cols = feature(slot, other)

            @pl.loop(0, 2)
            def _(h):
                w = weights[b, slot + 4 * other, parts[2], :]
                late_acc[h] += mm(rows_of(cots, h, cols), w, NT)

        def down_block(b):
            late_acc[...] = jnp.zeros_like(late_acc)

            @pl.loop(0, 8)
            def _(i):
                take_part(b, 2, i // 2, i % 2)
                down_shard(b, i // 2, i % 2)

        def pieces_block(h):
            @pl.loop(0, TP)
            def _(m):
                at = pl.ds(pl.multiple_of(m * half, half), half)
                to = pl.ds(pl.multiple_of(h * half, half), half)
                gate, up = acc[0, h, at, :], acc[1, h, at, :]
                grad = 0.5 * late_acc[h, at, :]
                sig = 1.0 / (1.0 + jnp.exp(-gate))
                act = gate * sig
                turn = sig * (1.0 + gate * (1.0 - sig))
                pieces[0, m, to, :] = (grad * up * turn).astype(jnp.bfloat16)
                pieces[1, m, to, :] = (grad * act).astype(jnp.bfloat16)
                pieces[2, m, to, :] = (act * up).astype(jnp.bfloat16)

        def swaps(b):
            out = []
            for j in range(3):
                out.append(remote(pieces.at[j], pieces_in.at[j], sem(("x", b, j)), peer_dev))
            for k in range(2):
                cols = feature(k, 1)
                for j, src in enumerate((normed, acts.at[2 * b + 1])):
                    out.append(
                        remote(src.at[:, :, cols], cols_in.at[j, k], sem(("y", b, j, k)), peer_dev)
                    )
            return out

        def part_copy(r, m):
            at = pl.ds(r * q, q)
            return remote(
                part.at[m, at], part_in1.at[m - 1, at], sem(("n", r, m)),
                device(z, core, column(m)),
            )

        lanes = (pl.ds(0, normed.shape[2] // 2), pl.ds(normed.shape[2] // 2, normed.shape[2] // 2))

        def part_first(h, columns=(1, 2), kinds=(0, 1)):
            at = pl.ds(h * half, half)
            out = []
            for m in columns:
                for kind in kinds:
                    block, slot = ((m, m - 1), (3, 2))[kind]
                    out.append(
                        remote(
                            part.at[block, at, lanes[m - 1]], part_in2.at[slot, at, lanes[m - 1]],
                            sem(("o", h, m, slot)), device(z, core, column(m)),
                        )
                    )
            return out

        def part_second(h, columns=(1, 2)):
            at = pl.ds(h * half, half)
            return [
                remote(
                    part.at[3 - m, at, lanes[m - 1]], part_in2.at[2 - m, at, lanes[m - 1]],
                    sem(("t", h, m)), device(z, core, column(3 - m)),
                )
                for m in columns
            ]

        def part_merge(h):
            at = pl.ds(h * half, half)
            for m in (1, 2):
                part_first(h, (m,), (1,))[0].wait_recv()
                mine_too = part[3 - m, at, lanes[m - 1]].astype(jnp.float32)
                other = part_in2[2, at, lanes[m - 1]].astype(jnp.float32)
                part[3 - m, at, lanes[m - 1]] = (mine_too + other).astype(jnp.bfloat16)
                part_second(h, (m,))[0].start()

        def grad_part(b, h):
            at = pl.ds(h * half, half)

            @pl.loop(0, 8)
            def _(i):
                cols = feature(i % 4, i // 4)
                total = None
                for j in range(2):
                    left = pieces[j, :, at, :].reshape(tile, hidden)
                    one = mm(left, weights[b, i, parts[j], :], NN)
                    total = one if j == 0 else total + one
                part[:, at, cols] = total.astype(jnp.bfloat16).reshape(TP, half, width)

        def fold(b):
            for copy in swaps(b):
                copy.wait_recv()
            tokens = TP * rows
            cots = acts.at[2 * b + 1]
            for k in (1, 0):
                cols = feature(k, 0)
                out = (own_grads, sent)[k].at[b]
                sides = (
                    (normed[:, :, cols].reshape(tokens, width), cols_in[0, k].reshape(tokens, width)),
                    (cots[:, :, cols].reshape(tokens, width), cols_in[1, k].reshape(tokens, width)),
                )
                for j in range(3):
                    own, other = sides[j // 2]
                    one = mm(pieces[j].reshape(tokens, hidden), own, TN)
                    one = one + mm(pieces_in[j].reshape(tokens, hidden), other, TN)
                    out[j] = (one if j < 2 else 0.5 * one).astype(jnp.bfloat16)
                    if k == 1 and (b == 0 or j < 2):
                        grad_back(b, j).start()
            keep_grads(b).start()

        def keep_grads(b):
            return local(own_grads.at[b], grads[b], 25 + b)

        def keep_late(m):
            at = own_quarter(column(m))
            return local(late.at[1, m, pl.ds(0, q)], late_mid.at[at], 27 + m)

        def rows_grad(b, r, out):
            if b == 0:
                copies = part_first(r, kinds=(0,)) + part_second(r)
            else:
                copies = [part_copy(r, m) for m in range(1, TP)]
            for copy in copies:
                copy.wait_recv()
            arrived = (part_in2, part_in1)[b]
            size = half if b == 0 else q
            at = pl.ds(r * size, size)
            total = part[0, at, :].astype(jnp.float32)
            for m in range(1, 3 if b == 0 else TP):
                total = total + arrived[m - 1, at, :].astype(jnp.float32)
            wide, factor = norm_parts(acts[2 * b, 0, at, :])
            scaled = total * gains[b][...]
            unit = wide * factor
            inner_mean = jnp.mean(scaled * unit, axis=-1, keepdims=True)
            cot = acts[2 * b + 1, 0, at, :].astype(jnp.float32)
            out[at, :] = (cot + factor * (scaled - unit * inner_mean)).astype(jnp.bfloat16)

        def mid_copy(h, m):
            at = pl.ds(h * half, half)
            return remote(
                acts.at[3, 0, at], acts.at[3, m, at], sem(("a", h, m)),
                device(z, core, column(m)),
            )

        def mid_forward(h, m):
            at = pl.ds(h * half + (m - 1) * q, q)
            return remote(
                acts.at[3, m, at], acts.at[3, 3, at], sem(("f", h, m)),
                device(z, core, column(3 - m)),
            )

        def mid_pass(h):
            for m in (1, 2):
                mid_copy(h, m).wait_recv()
                mid_forward(h, m).start()

        def late_block(b, n):
            @pl.loop(0, TP * 2)
            def _(i):
                at = pl.ds(pl.multiple_of((i % 2) * q, q), q)
                wide, factor = norm_parts(late[n, i // 2, at, :])
                late_normed[i // 2, at, :] = (wide * factor * gains[b][...]).astype(jnp.bfloat16)

            late_acc[...] = jnp.zeros_like(late_acc)

            @pl.loop(0, 8)
            def _(i):
                cols = feature(i % 4, i // 4)
                piece = late_normed[:, :, cols].reshape(tile, width)
                for j in range(2):
                    late_acc[j] += mm(piece, weights[b, i, parts[j], :], NT)

            gate = late_acc[0]
            hid = (gate / (1.0 + jnp.exp(-gate)) * late_acc[1]).astype(jnp.bfloat16)
            late_hid[...] = hid
            if n == 0:
                late_acc[...] = jnp.zeros_like(late_acc)
                for h in range(2):
                    for m in (1, 2):
                        mid_forward(h, m).wait_recv()

            @pl.loop(0, 8)
            def _(i):
                slot, other = i // 2, i % 2
                if n == 0:
                    take_part(b, 2, slot, other)
                cols = feature(slot, other)
                w = weights[b, slot + 4 * other, parts[2], :]
                one = mm(late_hid[...], w, NN).astype(jnp.bfloat16)
                late_part[:, :, cols] = one.reshape(TP, half, width)
                if n == 0:
                    for m in range(1, TP):
                        late_block_copy(i, m).start()
                    down_shard(b, slot, other)

            if n == 1:
                for r in (1, 0):
                    for m in range(1, TP):
                        late_copy(r, m).start()

        late_base = sem(("b", 0))
        for i in range(1, 24):
            sem(("b", i))

        def late_block_copy(i, m):
            cols = feature(i // 2, i % 2)
            return remote(
                late_part.at[m, :, cols], late_part_in.at[0, m - 1, :, cols],
                late_base + i * 3 + (m - 1), device(z, core, column(m)),
            )

        def late_copy(r, m):
            at = pl.ds(r * q, q)
            return remote(
                late_part.at[m, at], late_part_in.at[1, m - 1, at], sem(("h", r, m)),
                device(z, core, column(m)),
            )

        def late_sum(n, r, out):
            if n == 1:
                for m in range(1, TP):
                    late_copy(r, m).wait_recv()
            at = pl.ds(r * q, q)
            total = late_part[0, at, :].astype(jnp.float32)
            for m in range(1, TP):
                total = total + late_part_in[n, m - 1, at, :].astype(jnp.float32)
            value = late[n, 0, at, :].astype(jnp.float32) + 0.5 * total
            out[at, :] = value.astype(jnp.bfloat16)

        def late_spread(m):
            return remote(
                late.at[1, 0], late.at[1, m], sem(("k", m)), device(z, core, column(m))
            )

        def late_forward(m):
            at = pl.ds((m - 1) * q, q)
            return remote(
                late.at[1, m, at], late.at[1, 3, at], sem(("j", m)), device(z, core, column(3 - m))
            )

        rows_ready(0)
        normalize_block(0)
        pre_block(0, 0, 8)
        rows_ready(1)
        gather_rows(2, 4)
        gather_rows(3, 5)
        down_block(0)
        for h in range(2):
            pieces_block(h)
            grad_part(0, h)
            for copy in part_first(h):
                copy.start()
        for copy in swaps(0):
            copy.start()
        part_merge(0)
        fold(0)
        part_merge(1)
        for copy in swaps(0):
            copy.wait_send()
        pl.semaphore_signal(ack, inc=1, device_id=peer_dev, device_id_type=pl.DeviceIdType.MESH)

        rows_ready(2)
        normalize_block(1)
        for h in range(2):
            rows_grad(0, h, acts.at[3, 0])
            for m in (1, 2):
                mid_copy(h, m).start()
            pre_block(1, 2 * h, 2 + 3 * h)
        mid_pass(0)
        mid_pass(1)
        pre_block(1, 5, 8)
        rows_ready(3)
        late_block(1, 0)

        @pl.loop(0, 2)
        def _(h):
            pieces_block(h)

        pl.semaphore_wait(ack, 1)
        for copy in swaps(1):
            copy.start()

        @pl.loop(0, 8)
        def _(i):
            for m in range(1, TP):
                late_block_copy(i, m).wait_recv()

        late_rows = late.at[1, 0]
        late_sum(0, 1, late_rows)
        late_sum(0, 0, late_rows)
        for m in (1, 2):
            late_spread(m).start()
        rows_back(0).start()
        for h in range(2):
            for copy in part_first(h) + part_second(h):
                copy.wait_send()
        grad_part(1, 0)
        for m in (1, 2):
            late_spread(m).wait_recv()
            late_forward(m).start()
        for r in (1, 0):
            for m in range(1, TP):
                part_copy(r, m).start()
        fold(1)

        @pl.loop(0, 8)
        def _(i):
            for m in range(1, TP):
                late_block_copy(i, m).wait_send()

        for m in (1, 2):
            late_forward(m).wait_recv()
        late_block(0, 1)
        for m in range(TP):
            keep_late(m).start()

        def finish(k):
            src = row_source(k).at[pl.ds(0, q)]
            for m in range(1, TP):
                deliver(k, m, src).start()
            keep_rows(k, src).start()

        rows_grad(1, 1, done_rows.at[1])
        rows_back(2).start()
        rows_grad(1, 0, done_rows.at[1])
        late_sum(1, 1, done_rows.at[0])
        rows_back(1).start()
        grad_back(1, 2).start()
        finish(2)
        late_sum(1, 0, done_rows.at[0])
        finish(1)

        for copy in inner_sends():
            copy.wait_send()
        for b in range(2):
            for j in range(3):
                for s in range(4):
                    src = shards[b][j] if s == 0 else weights.at[b, s, parts[j]]
                    shard_forward(b, j, s, src).wait_send()
                grad_back(b, j).wait_send()
        for a in range(4):
            for copy in spread_rows(a):
                copy.wait_send()
        for copy in swaps(1):
            copy.wait_send()
        for m in range(1, TP):
            for r in range(2):
                part_copy(r, m).wait_send()
                late_copy(r, m).wait_send()
        for m in (1, 2):
            late_spread(m).wait_send()
            late_forward(m).wait_send()
            for h in range(2):
                mid_copy(h, m).wait_send()
                mid_forward(h, m).wait_send()
        for b in range(2):
            keep_grads(b).wait()
        for m in range(TP):
            keep_late(m).wait()
        for k in range(3):
            rows_back(k).wait_send()
            if k > 0:
                keep_rows(k, row_source(k).at[pl.ds(0, q)]).wait()
                for m in range(1, TP):
                    deliver(k, m, row_source(k).at[pl.ds(0, q)]).wait_send()
                    deliver_wait(k, m)


def add_kernel(r0, r1, r2, grads2, grads1, *refs):
    olds, outs = refs[:6], refs[6:]
    for src, dst in zip((r0, r1, r2), outs[:3]):
        dst[...] = src[...]
    for j in range(6):
        grads = (grads1, grads2)[j // 3]
        outs[3 + j][...] = olds[j][...] + grads[j % 3].astype(jnp.float32)


def per_device(
    late_input,
    early_input,
    early_mid,
    cotangent,
    gain_first,
    gain_second,
    gate_first,
    up_first,
    down_first,
    gate_second,
    up_second,
    down_second,
    *sums,
):
    count, feats = late_input.shape
    width, hidden = gate_first.shape
    q = count // TP
    half = 2 * q
    tile = TP * half
    bf = jnp.bfloat16
    anywhere = pl.BlockSpec(memory_space=pl.ANY)
    in_vmem = pl.BlockSpec(memory_space=pltpu.VMEM)
    rows_shape = jax.ShapeDtypeStruct((count, feats), bf)
    grads_shape = jax.ShapeDtypeStruct((3, hidden, width), bf)
    outs = pl.pallas_call(
        step_kernel,
        out_shape=[rows_shape] * 3 + [grads_shape] * 2,
        in_specs=[anywhere] * 4 + [in_vmem] * 2 + [anywhere] * 6,
        out_specs=[anywhere] * 5,
        scratch_shapes=[
            pltpu.VMEM((2, 8, 3 * hidden, width), bf),
            pltpu.VMEM((4, TP, count, feats), bf),
            pltpu.VMEM((2, TP, half, feats), bf),
            pltpu.VMEM((TP, count, feats), bf),
            pltpu.VMEM((TP, half, feats), bf),
            pltpu.VMEM((3, TP, count, hidden), bf),
            pltpu.VMEM((3, TP, count, hidden), bf),
            pltpu.VMEM((2, 2, TP, count, width), bf),
            pltpu.VMEM((TP, count, feats), bf),
            pltpu.VMEM((3, count, feats), bf),
            pltpu.VMEM((3, half, feats), bf),
            pltpu.VMEM((TP, half, feats), bf),
            pltpu.VMEM((2, 3, half, feats), bf),
            pltpu.VMEM((2, 3, hidden, width), bf),
            pltpu.VMEM((3, q, feats), bf),
            pltpu.VMEM((2, half, feats), bf),
            pltpu.VMEM((2, 3, hidden, width), bf),
            pltpu.VMEM((2, 2, tile, hidden), jnp.float32),
            pltpu.VMEM((2, tile, hidden), jnp.float32),
            pltpu.VMEM((tile, hidden), bf),
            pltpu.SemaphoreType.DMA((208,)),
            pltpu.SemaphoreType.DMA((208,)),
            pltpu.SemaphoreType.DMA((31,)),
            pltpu.SemaphoreType.REGULAR,
        ],
        compiler_params=pltpu.CompilerParams(
            collective_id=0, has_side_effects=True, vmem_limit_bytes=67043328
        ),
        name="step",
    )(
        late_input, early_mid, cotangent, early_input,
        gain_second.reshape((1, -1)), gain_first.reshape((1, -1)),
        gate_second.T, up_second.T, down_second,
        gate_first.T, up_first.T, down_first,
    )
    tall = [old.T if j % 3 < 2 else old for j, old in enumerate(sums)]
    steps = 2
    row_spec = pl.BlockSpec((count // steps, feats), lambda i: (i, 0))
    sum_spec = pl.BlockSpec((hidden // steps, width), lambda i: (i, 0))
    grad_spec = pl.BlockSpec((3, hidden // steps, width), lambda i: (0, i, 0))
    done = pl.pallas_call(
        add_kernel,
        grid=(steps,),
        out_shape=[rows_shape] * 3 + [jax.ShapeDtypeStruct((hidden, width), jnp.float32)] * 6,
        in_specs=[row_spec] * 3 + [grad_spec] * 2 + [sum_spec] * 6,
        out_specs=[row_spec] * 3 + [sum_spec] * 6,
        name="add",
    )(*outs, *tall)
    fresh = [new.T if j % 3 < 2 else new for j, new in enumerate(done[3:])]
    return tuple(done[:3]) + tuple(fresh)


def normalize(values, gain_vector):
    widened = values.astype(jnp.float32)
    factor = lax.rsqrt(jnp.mean(widened * widened, axis=-1, keepdims=True) + norm_eps)
    normed = (widened * factor * gain_vector).astype(jnp.bfloat16)
    return (widened, factor, normed)


def project(rows, weights):
    return jnp.dot(rows, weights, preferred_element_type=jnp.float32)


def project_back(hidden_rows, weights):
    return jnp.einsum("tf,df->td", hidden_rows, weights, preferred_element_type=jnp.float32)


def fold_rows(left, right):
    return jnp.einsum("ta,tb->ab", left, right, preferred_element_type=jnp.float32)


def own_rows(rows):
    count = rows.shape[0] // lax.axis_size("tp")
    return lax.dynamic_slice_in_dim(rows, lax.axis_index("tp") * count, count, axis=0)


def sum_rows(partial):
    shares = lax.all_to_all(
        partial.astype(jnp.bfloat16), "tp", split_axis=0, concat_axis=0, tiled=True
    )
    shares = shares.reshape((lax.axis_size("tp"), -1, shares.shape[1]))
    return jnp.sum(shares.astype(jnp.float32), axis=0)


def join_rows(rows):
    return lax.all_gather(rows, "tp", axis=0, tiled=True)


def block_forward(values, gain_vector, weights, width):
    widened, factor, normed = normalize(values, gain_vector)
    pre = project(normed, weights[:, : 2 * width])
    hidden = (jax.nn.silu(pre[:, :width]) * pre[:, width:]).astype(jnp.bfloat16)
    branch = sum_rows(project_back(hidden, weights[:, 2 * width :]))
    return join_rows((own_rows(widened) + 0.5 * branch).astype(jnp.bfloat16))


def block_backward(normalized, cotangent, weights, width):
    widened, factor, normed = normalized
    pre = project(normed, weights[:, : 2 * width])
    gate_pre, up_pre = pre[:, :width], pre[:, width:]
    sigmoid_gate = jax.nn.sigmoid(gate_pre)
    activated = gate_pre * sigmoid_gate
    hidden = (activated * up_pre).astype(jnp.bfloat16)
    hidden_grad = 0.5 * project(cotangent, weights[:, 2 * width :])
    gate_grad = (
        hidden_grad * up_pre * sigmoid_gate * (1.0 + gate_pre * (1.0 - sigmoid_gate))
    ).astype(jnp.bfloat16)
    up_grad = (hidden_grad * activated).astype(jnp.bfloat16)
    pieces = jnp.concatenate((gate_grad, up_grad, hidden), axis=1)
    partial_value = project_back(pieces[:, : 2 * width], weights[:, : 2 * width])
    return (partial_value, pieces)


def backward_rows(normalized, cotangent, gain_vector, partial_value):
    normed_grad = sum_rows(partial_value)
    widened, factor = own_rows(normalized[0]), own_rows(normalized[1])
    scaled = normed_grad * gain_vector
    unit_rows = widened * factor
    rows_grad = own_rows(cotangent).astype(jnp.float32) + factor * (
        scaled - unit_rows * jnp.mean(scaled * unit_rows, axis=-1, keepdims=True)
    )
    return rows_grad.astype(jnp.bfloat16)


def gather_weights(gate, up, down):
    return lax.all_gather(jnp.concatenate((gate, up, down.T), axis=1), "fs", axis=0, tiled=True)


def share_columns(rows):
    return lax.all_to_all(rows, "fs", split_axis=1, concat_axis=0, tiled=True)


def join_columns(share):
    joined = join_rows(share)
    parts = joined.reshape((lax.axis_size("tp"), lax.axis_size("fs"), -1, joined.shape[1]))
    return jnp.swapaxes(parts, 0, 1).reshape(joined.shape)


def per_device_general(
    late_input,
    early_input,
    early_mid,
    cotangent,
    gain_first,
    gain_second,
    gate_first,
    up_first,
    down_first,
    gate_second,
    up_second,
    down_second,
    sum_gate_first,
    sum_up_first,
    sum_down_first,
    sum_gate_second,
    sum_up_second,
    sum_down_second,
):
    width = gate_first.shape[1]
    weights_second = gather_weights(gate_second, up_second, down_second)
    weights_first = gather_weights(gate_first, up_first, down_first)
    norm_second = normalize(early_mid, gain_second)
    norm_first = normalize(early_input, gain_first)
    early_rows = jnp.stack(
        (own_rows(norm_second[2]), own_rows(norm_first[2]), own_rows(cotangent))
    )
    early_shares = lax.all_to_all(early_rows, "fs", split_axis=2, concat_axis=1, tiled=True)
    columns_second = join_columns(early_shares[0])
    columns_first = join_columns(early_shares[1])
    columns_cotangent = join_columns(early_shares[2])
    partial_second, pieces_second = block_backward(
        norm_second, cotangent, weights_second, width
    )
    all_second = lax.all_gather(pieces_second, "fs", axis=0, tiled=True)
    mid_rows = backward_rows(norm_second, cotangent, gain_second, partial_second)
    mid_grad = join_rows(mid_rows)
    columns_mid = join_columns(share_columns(mid_rows))
    partial_first, pieces_first = block_backward(norm_first, mid_grad, weights_first, width)
    all_first = lax.all_gather(pieces_first, "fs", axis=0, tiled=True)
    late_mid = block_forward(late_input, gain_first, weights_first, width)
    input_grad = join_rows(backward_rows(norm_first, mid_grad, gain_first, partial_first))
    late_out = block_forward(late_mid, gain_second, weights_second, width)

    def collect(pieces, columns_in, columns_out, sums):
        return (
            sums[0] + fold_rows(columns_in, pieces[:, :width]),
            sums[1] + fold_rows(columns_in, pieces[:, width : 2 * width]),
            sums[2] + 0.5 * fold_rows(pieces[:, 2 * width :], columns_out),
        )

    new_second = collect(
        all_second, columns_second, columns_cotangent, (sum_gate_second, sum_up_second, sum_down_second)
    )
    new_first = collect(
        all_first, columns_first, columns_mid, (sum_gate_first, sum_up_first, sum_down_first)
    )
    return (late_mid, late_out, input_grad) + new_first + new_second


def solution(mesh):
    rows, up_down, down_up = P("fs", None), P("fs", "tp"), P("tp", "fs")
    weights = (up_down, up_down, down_up)
    in_specs = (rows,) * 4 + (P(), P()) + weights * 4
    out_specs = (rows,) * 3 + weights * 2
    line_of_four = mesh.shape["fs"] == PLANES * CORES and mesh.shape["tp"] == TP
    body = per_device if line_of_four else per_device_general
    return jax.shard_map(
        body, mesh=mesh, in_specs=in_specs, out_specs=out_specs, check_vma=False
    )
```
